128 devices in a mesh: ep: 128 (over z, y, x, core).
Axes of the slice: x: 4, y: 4, z: 4, core: 2. Of those that a mesh axis runs over, the one named last changes fastest.
Arguments:
- tokens: bfloat16 [2048, 1024], P('ep'), may hold values from -6 to 6
- lengths: int32 [2048], P('ep'), may hold values from 1 to 8191
- cache_keys: bfloat16 [2048, 128, 512], P('ep'), may hold values from -6 to 6
- cache_values: bfloat16 [2048, 128, 1024], P('ep'), may hold values from -6 to 6
- retention_state: float32 [2048, 4, 128, 256], P('ep'), may hold values from -24 to 24
- mix_gain: float32 [1024], replicated, may hold values from 0.1 to 1.9
- query_weight: bfloat16 [1024, 512], replicated, may hold values from -0.1875 to 0.1875
- key_weight: bfloat16 [1024, 512], replicated, may hold values from -0.1875 to 0.1875
- value_weight: bfloat16 [1024, 1024], replicated, may hold values from -0.1875 to 0.1875
- out_weight: bfloat16 [1024, 1024], replicated, may hold values from -0.1875 to 0.1875
- ffn_gain: float32 [1024], replicated, may hold values from 0.1 to 1.9
- routes: int32 [2048, 6], P('ep'), may hold values from 0 to 127, all different within a row; in each aligned block of 16 rows (0 to 15, 16 to 31, ...) at most 2 rows name the same one
- route_scores: float32 [2048, 6], P('ep'), may hold values from 0.05 to 1
- expert_gate: bfloat16 [128, 1024, 256], P('ep'), may hold values from -0.1875 to 0.1875
- expert_up: bfloat16 [128, 1024, 256], P('ep'), may hold values from -0.1875 to 0.1875
- expert_down: bfloat16 [128, 256, 1024], P('ep'), may hold values from -0.375 to 0.375
- shared_gate: bfloat16 [1024, 256], replicated, may hold values from -0.1875 to 0.1875
- shared_up: bfloat16 [1024, 256], replicated, may hold values from -0.1875 to 0.1875
- shared_down: bfloat16 [256, 1024], replicated, may hold values from -0.375 to 0.375
- dense_gate: bfloat16 [4096, 1024], P('ep'), may hold values from -0.1875 to 0.1875
- dense_up: bfloat16 [4096, 1024], P('ep'), may hold values from -0.1875 to 0.1875
- dense_down: bfloat16 [4096, 1024], P('ep'), may hold values from -0.09375 to 0.09375
- dense_mix: float32 [1024], replicated, may hold values from -3 to 3
Outputs:
- layer_out: bfloat16 [2048, 1024], P('ep')
- new_keys: bfloat16 [2048, 512], P('ep')
- new_values: bfloat16 [2048, 1024], P('ep')
The draws below stay inside these ranges and needn't reach their ends.
Inputs may be any that keep to these rules, and one draw needn't show every extreme that they name: `routes`: each row names 6 different experts; among the rows of one device no expert is named more than 2 times.
All inputs are finite; a program needn't handle non-finite values.
Results may differ from the reference program's by a relative error of at most 0.012.
Values may be sent and summed in bfloat16 or wider, within the bound.
A program may use at most 128 MiB of HBM per device.

```python
import math
import jax
import jax.numpy as jnp
import numpy as np
from jax import lax

D = 1024
HEADS = 4
DK = 128
DV = 256
BLOCK = 128
SEQ_DEV = 16
SEQS = 2048
EXPERTS = 128
TOP_K = 6
CAP = 2
EH = 256
SH = 256
DENSE_FF = 4096
N_EP = 128


def plant(values, stream_key, smallest, top_value):
    dims = values.shape
    spot = [jax.random.randint(jax.random.fold_in(stream_key, axis), (), 0, dims[axis]) for axis in range(len(dims))]
    values = values.at[tuple(spot)].set(smallest)
    longest = dims.index(max(dims))
    spot[longest] = (spot[longest] + 1) % dims[longest]
    return values.at[tuple(spot)].set(top_value)


def shard_levels(rng, dims, shards, low, high):
    factor_of = 1.0
    for axis_at, shards_of in shards:
        heights = jax.random.uniform(jax.random.fold_in(jax.random.fold_in(rng, 6), axis_at), (shards_of,), jnp.float32, low / len(shards), high / len(shards))
        factor_of = factor_of * jnp.repeat(jnp.exp(heights), dims[axis_at] // shards_of).reshape((-1,) + (1,) * (len(dims) - 1 - axis_at))
    return factor_of


def routed_block(key, own, number, rows, count, top, reach, slope):
    sequence = jax.random.permutation(key, count)
    crowded, common = portions_of(count, rows * top, reach, slope, True), portions_of(count, rows * top, reach, slope, False)
    places = jnp.arange(count)

    def named(tallies, offset_by):
        used = int((tallies > 0).sum())
        fixed = max(1, used // 4)
        passed = fixed + (places - fixed + offset_by * (used - fixed)) % max(1, count - fixed)
        return jnp.zeros((count,), jnp.int32).at[sequence[jnp.where(places < fixed, places, passed)]].set(jnp.asarray(tallies, jnp.int32))

    tallies = jnp.where(number % 4 == 0, named(crowded, number // 4), named(common, number - number // 4 - 1))
    mixed = jax.random.permutation(jax.random.fold_in(own, 3), count)
    donor, receiver = mixed[0:count // 2 * 2:2], mixed[1:count // 2 * 2:2]
    room = jnp.minimum(tallies[donor] - 1, reach - tallies[receiver]) // 2
    room = jnp.where((donor == sequence[0]) | (receiver == sequence[0]) | (tallies[receiver] == 0), 0, jnp.maximum(room, 0))
    passed = jax.random.randint(jax.random.fold_in(own, 4), (count // 2,), 0, 1 << 20) % (room + 1)
    tallies = tallies.at[donor].add(-passed).at[receiver].add(passed)
    members = jnp.searchsorted(jnp.cumsum(tallies), jnp.arange(rows * top), side="right").astype(jnp.int32)
    grid = members.reshape(top, rows).T
    grid = grid[jax.random.permutation(jax.random.fold_in(own, 1), rows)]
    offset_by = jax.random.randint(jax.random.fold_in(own, 2), (rows, 1), 0, top)
    return jnp.take_along_axis(grid, (jnp.arange(top)[None, :] + offset_by) % top, axis=1)


def portions_of(amount, total, limit, slope, full):
    portions = [(1 << 20) // math.isqrt(grade ** slope) + 1 for grade in range(1, amount + 1)]
    largest = limit if full else min(limit, max(-(-total // amount), total * portions[0] // sum(portions)))
    least = 1 if total - largest >= amount - 1 else 0
    counts, surplus = [largest] + [least] * (amount - 1), total - largest - least * (amount - 1)
    while surplus > 0:
        free = [i for i in range(1, amount) if counts[i] < largest] or [i for i in range(1, amount) if counts[i] < limit]
        pool, budget = sum([portions[i] for i in free]), surplus
        for i in free:
            addition = min(limit - counts[i], max(1, budget * portions[i] // pool), surplus)
            counts[i] = counts[i] + addition
            surplus = surplus - addition
    return np.array(counts)


def gaussian(own_key, dims, deviation, reach, shards=(), held_as=jnp.bfloat16):
    result = deviation * jax.random.normal(own_key, dims, jnp.float32)
    if shards:
        result = result * shard_levels(own_key, dims, shards, -0.22, 0.18)
    return jnp.clip(result, -reach, reach).astype(held_as)


def setup_inputs(seed: int = 0) -> dict:
    key_of = jax.random.split(jax.random.key(seed), 24)
    tokens = gaussian(key_of[0], (SEQS, D), 1.0, 6.0, ((0, 128),))
    lengths = plant(jax.random.randint(key_of[1], (SEQS,), 1, 8192), jax.random.fold_in(key_of[1], 1), 1, 8191).astype(jnp.int32)
    cache_keys = gaussian(key_of[2], (SEQS, BLOCK, HEADS * DK), 1.0, 6.0, ((0, 128),))
    cache_values = gaussian(key_of[3], (SEQS, BLOCK, HEADS * DV), 1.0, 6.0, ((0, 128),))
    retention_state = gaussian(key_of[4], (SEQS, HEADS, DK, DV), 4.0, 24.0, ((0, 128),), jnp.float32)
    mix_gain = jnp.clip(1.0 + 0.18 * jax.random.normal(key_of[5], (D,), jnp.float32), 0.1, 1.9)
    query_weight = gaussian(key_of[6], (D, HEADS * DK), D ** -0.5, 0.1875)
    key_weight = gaussian(key_of[7], (D, HEADS * DK), D ** -0.5, 0.1875)
    value_weight = gaussian(key_of[8], (D, HEADS * DV), D ** -0.5, 0.1875)
    out_weight = gaussian(key_of[9], (HEADS * DV, D), (HEADS * DV) ** -0.5, 0.1875)
    ffn_gain = jnp.clip(1.0 + 0.18 * jax.random.normal(key_of[10], (D,), jnp.float32), 0.1, 1.9)
    routes_keys = jax.random.split(jax.random.fold_in(key_of[11], 1), SEQS // SEQ_DEV)
    routes_turns = jax.random.permutation(jax.random.fold_in(key_of[11], 3), SEQS // SEQ_DEV)
    routes = jax.vmap(lambda own, number: routed_block(jax.random.fold_in(key_of[11], 2), own, number, SEQ_DEV, EXPERTS, TOP_K, CAP, 1))(routes_keys, routes_turns).reshape((SEQS, TOP_K))
    route_scores = jnp.clip(0.05 + 0.95 * jax.random.uniform(key_of[12], (SEQS, TOP_K), jnp.float32) ** shard_levels(key_of[12], (SEQS, TOP_K), ((0, 128),), -0.2, 0.2), 0.05, 1.0)
    expert_gate = gaussian(key_of[13], (EXPERTS, D, EH), D ** -0.5, 0.1875, ((0, 128),))
    expert_up = gaussian(key_of[14], (EXPERTS, D, EH), D ** -0.5, 0.1875, ((0, 128),))
    expert_down = gaussian(key_of[15], (EXPERTS, EH, D), EH ** -0.5, 0.375, ((0, 128),))
    shared_gate = gaussian(key_of[16], (D, SH), D ** -0.5, 0.1875)
    shared_up = gaussian(key_of[17], (D, SH), D ** -0.5, 0.1875)
    shared_down = gaussian(key_of[18], (SH, D), SH ** -0.5, 0.375)
    dense_gate = gaussian(key_of[19], (DENSE_FF, D), D ** -0.5, 0.1875, ((0, 128),))
    dense_up = gaussian(key_of[20], (DENSE_FF, D), D ** -0.5, 0.1875, ((0, 128),))
    dense_down = gaussian(key_of[21], (DENSE_FF, D), DENSE_FF ** -0.5, 0.09375, ((0, 128),))
    dense_mix = jnp.clip(jax.random.uniform(key_of[22], (D,), jnp.float32, -3.0, 3.0), -3.0, 3.0)
    return {"tokens": tokens, "lengths": lengths, "cache_keys": cache_keys, "cache_values": cache_values, "retention_state": retention_state, "mix_gain": mix_gain, "query_weight": query_weight, "key_weight": key_weight, "value_weight": value_weight, "out_weight": out_weight, "ffn_gain": ffn_gain, "routes": routes, "route_scores": route_scores, "expert_gate": expert_gate, "expert_up": expert_up, "expert_down": expert_down, "shared_gate": shared_gate, "shared_up": shared_up, "shared_down": shared_down, "dense_gate": dense_gate, "dense_up": dense_up, "dense_down": dense_down, "dense_mix": dense_mix}


eps = 1e-06
route_scale = 2.5
rope_base = 10000.0

def normed(values):
    return values * lax.rsqrt(lax.optimization_barrier(jnp.mean(values * values, axis=-1, keepdims=True)) + eps)

def log_decay(head_count):
    return jnp.log1p(-jnp.exp2(-5.0 - jnp.arange(head_count, dtype=jnp.float32)))

def rotate(values, positions):
    half_size = values.shape[-1] // 2
    inverse = rope_base ** (-jnp.arange(half_size, dtype=jnp.float32) / half_size)
    angles = positions.astype(jnp.float32)[:, None, None] * inverse[None, None, :]
    cosine = jnp.cos(angles)
    sine_part = jnp.sin(angles)
    first_half = values[..., :half_size]
    second = values[..., half_size:]
    return jnp.concatenate([first_half * cosine - second * sine_part, first_half * sine_part + second * cosine], axis=-1)

def swiglu(inputs, w_gate, w_up, w_down):
    gate_part = jnp.dot(inputs, w_gate, preferred_element_type=jnp.float32)
    up_part = jnp.dot(inputs, w_up, preferred_element_type=jnp.float32)
    hidden = (jax.nn.silu(gate_part) * up_part).astype(jnp.bfloat16)
    return jnp.dot(hidden, w_down, preferred_element_type=jnp.float32)

def retain(tokens, lengths, mix_gain, w_query, w_key, w_value, w_out, cache_keys, cache_values, carry_state):
    seq_count, head_count, key_size, value_size = carry_state.shape
    block_size = cache_keys.shape[1]
    widened = tokens.astype(jnp.float32)
    normal_in = (normed(widened) * mix_gain).astype(jnp.bfloat16)
    raw_query = jnp.dot(normal_in, w_query, preferred_element_type=jnp.float32).reshape(seq_count, head_count, key_size)
    raw_key = jnp.dot(normal_in, w_key, preferred_element_type=jnp.float32).reshape(seq_count, head_count, key_size)
    raw_value = jnp.dot(normal_in, w_value, preferred_element_type=jnp.float32).reshape(seq_count, head_count, value_size)
    queries = (rotate(raw_query, lengths) * key_size ** (-0.5)).astype(jnp.bfloat16)
    new_keys = rotate(raw_key, lengths).astype(jnp.bfloat16)
    new_values = raw_value.astype(jnp.bfloat16)
    filled = lengths % block_size
    decay_rate = log_decay(head_count)
    places = jnp.arange(block_size, dtype=jnp.int32)
    stored_keys = cache_keys.reshape(seq_count, block_size, head_count, key_size)
    stored_values = cache_values.reshape(seq_count, block_size, head_count, value_size)
    scores = jnp.einsum('shd,sjhd->shj', queries.astype(jnp.float32), stored_keys.astype(jnp.float32))
    distance = jnp.maximum(filled[:, None] - places[None, :], 0).astype(jnp.float32)
    live_mask = places[None, :] < filled[:, None]
    weighted = jnp.where(live_mask[:, None, :], scores * jnp.exp(distance[:, None, :] * decay_rate[None, :, None]), 0.0).astype(jnp.bfloat16)
    own_weight = lax.optimization_barrier(jnp.sum(queries.astype(jnp.float32) * new_keys.astype(jnp.float32), axis=-1)).astype(jnp.bfloat16)
    inside = jnp.einsum('shj,sjhe->she', weighted.astype(jnp.float32), stored_values.astype(jnp.float32))
    inside = inside + own_weight.astype(jnp.float32)[:, :, None] * new_values.astype(jnp.float32)
    carried = jnp.einsum('shd,shde->she', queries.astype(jnp.float32), carry_state, precision=lax.Precision.HIGHEST)
    carried = carried * jnp.exp((filled.astype(jnp.float32)[:, None] + 1.0) * decay_rate[None, :])[:, :, None]
    headed = normed(inside + carried).astype(jnp.bfloat16).reshape(seq_count, head_count * value_size)
    mixer_out = jnp.dot(headed, w_out, preferred_element_type=jnp.float32)
    residual = widened + normed(mixer_out)
    return (residual, new_keys.reshape(seq_count, head_count * key_size), new_values.reshape(seq_count, head_count * value_size))

def reference(tokens, lengths, cache_keys, cache_values, retention_state, mix_gain, query_weight, key_weight, value_weight, out_weight, ffn_gain, routes, route_scores, expert_gate, expert_up, expert_down, shared_gate, shared_up, shared_down, dense_gate, dense_up, dense_down, dense_mix):
    residual, new_keys, new_values = retain(tokens, lengths, mix_gain, query_weight, key_weight, value_weight, out_weight, cache_keys, cache_values, retention_state)
    normal_ffn = (normed(residual) * ffn_gain).astype(jnp.bfloat16)
    shared_out = swiglu(normal_ffn, shared_gate, shared_up, shared_down)
    dense_gate_part = jnp.dot(normal_ffn, dense_gate.T, preferred_element_type=jnp.float32)
    dense_up_part = jnp.dot(normal_ffn, dense_up.T, preferred_element_type=jnp.float32)
    dense_hidden = (jax.nn.silu(dense_gate_part) * dense_up_part).astype(jnp.bfloat16)
    dense_out = jnp.dot(dense_hidden, dense_down, preferred_element_type=jnp.float32)
    route_weight = route_scores / lax.optimization_barrier(jnp.sum(route_scores, axis=-1, keepdims=True)) * route_scale
    flat_routes = routes.reshape(-1)
    flat_weight = route_weight.reshape(-1)
    most_rows = N_EP * CAP
    slot_rank = jnp.arange(most_rows, dtype=jnp.int32)

    def one_expert(running, expert_id):
        hits = flat_routes == expert_id
        hit_count = jnp.sum(hits.astype(jnp.int32))
        picked = jnp.nonzero(hits, size=most_rows, fill_value=0)[0].astype(jnp.int32)
        is_valid = slot_rank < hit_count
        row_ids = picked // TOP_K
        outputs = swiglu(normal_ffn[row_ids], expert_gate[expert_id], expert_up[expert_id], expert_down[expert_id]).astype(jnp.bfloat16)
        added = jnp.where(is_valid[:, None], outputs.astype(jnp.float32) * flat_weight[picked][:, None], 0.0)
        return (running.at[row_ids].add(added), None)
    routed, _ = lax.scan(one_expert, jnp.zeros(residual.shape, jnp.float32), jnp.arange(EXPERTS, dtype=jnp.int32))
    combined = shared_out + routed + jax.nn.sigmoid(dense_mix) * dense_out
    layer_out = (residual + normed(combined)).astype(jnp.bfloat16)
    return (layer_out, new_keys, new_values)
```

```python
import functools

import jax
import jax.numpy as jnp
from jax import lax
from jax.experimental import pallas as pl
from jax.experimental.pallas import tpu as pltpu
from jax.sharding import PartitionSpec as P

eps = 1e-06
route_scale = 2.5
rope_base = 10000.0
MESH = pl.DeviceIdType.MESH
F32 = jnp.float32
BF16 = jnp.bfloat16
N_DEV = 128
TOKENS = 16
WIDTH = 1024
TOP = 6
STEP = 53


def normed(values):
    return values * lax.rsqrt(jnp.mean(values * values, axis=-1, keepdims=True) + eps)


def log_decay(head_count):
    return jnp.log1p(-jnp.exp2(-5.0 - jnp.arange(head_count, dtype=jnp.float32)))


def rotate(values, positions):
    half_size = values.shape[-1] // 2
    inverse = rope_base ** (-jnp.arange(half_size, dtype=jnp.float32) / half_size)
    angles = positions.astype(jnp.float32)[:, None, None] * inverse[None, None, :]
    cosine = jnp.cos(angles)
    sine_part = jnp.sin(angles)
    first_half = values[..., :half_size]
    second = values[..., half_size:]
    return jnp.concatenate(
        [first_half * cosine - second * sine_part, first_half * sine_part + second * cosine],
        axis=-1,
    )


def retain(
    tokens, lengths, mix_gain, w_query, w_key, w_value, w_out, cache_keys, cache_values, carry_state
):
    seq_count, head_count, key_size, value_size = carry_state.shape
    block_size = cache_keys.shape[1]
    widened = tokens.astype(jnp.float32)
    normal_in = (normed(widened) * mix_gain).astype(jnp.bfloat16)
    raw_query = jnp.dot(normal_in, w_query, preferred_element_type=jnp.float32).reshape(
        seq_count, head_count, key_size
    )
    raw_key = jnp.dot(normal_in, w_key, preferred_element_type=jnp.float32).reshape(
        seq_count, head_count, key_size
    )
    raw_value = jnp.dot(normal_in, w_value, preferred_element_type=jnp.float32).reshape(
        seq_count, head_count, value_size
    )
    queries = (rotate(raw_query, lengths) * key_size ** (-0.5)).astype(jnp.bfloat16)
    new_keys = rotate(raw_key, lengths).astype(jnp.bfloat16)
    new_values = raw_value.astype(jnp.bfloat16)
    filled = lengths % block_size
    decay_rate = log_decay(head_count)
    places = jnp.arange(block_size, dtype=jnp.int32)
    stored_keys = cache_keys.reshape(seq_count, block_size, head_count, key_size)
    stored_values = cache_values.reshape(seq_count, block_size, head_count, value_size)
    scores = jnp.einsum("shd,sjhd->shj", queries, stored_keys, preferred_element_type=jnp.float32)
    distance = jnp.maximum(filled[:, None] - places[None, :], 0).astype(jnp.float32)
    live_mask = places[None, :] < filled[:, None]
    weighted = jnp.where(
        live_mask[:, None, :],
        scores * jnp.exp(distance[:, None, :] * decay_rate[None, :, None]),
        0.0,
    ).astype(jnp.bfloat16)
    own_weight = jnp.sum(
        queries.astype(jnp.float32) * new_keys.astype(jnp.float32), axis=-1
    ).astype(jnp.bfloat16)
    inside = jnp.einsum(
        "shj,sjhe->she", weighted, stored_values, preferred_element_type=jnp.float32
    )
    inside = inside + own_weight.astype(jnp.float32)[:, :, None] * new_values.astype(jnp.float32)
    carried = jnp.einsum("shd,shde->she", queries.astype(jnp.float32), carry_state)
    carried = (
        carried
        * jnp.exp((filled.astype(jnp.float32)[:, None] + 1.0) * decay_rate[None, :])[:, :, None]
    )
    headed = (
        normed(inside + carried).astype(jnp.bfloat16).reshape(seq_count, head_count * value_size)
    )
    mixer_out = jnp.dot(headed, w_out, preferred_element_type=jnp.float32)
    residual = widened + normed(mixer_out)
    return (
        residual,
        new_keys.reshape(seq_count, head_count * key_size),
        new_values.reshape(seq_count, head_count * value_size),
    )


def dot(a, b):
    return jnp.dot(a, b, preferred_element_type=F32)


def dot_t(a, b):
    return lax.dot_general(a, b, (((1,), (1,)), ((), ())), preferred_element_type=F32)


def dot_0(a, b):
    return lax.dot_general(a, b, (((0,), (0,)), ((), ())), preferred_element_type=F32)


def silu(v):
    return v / (1.0 + jnp.exp(-v))


def iota(shape, dim):
    return lax.broadcasted_iota(jnp.int32, shape, dim)


def one_hot(mask):
    return jnp.where(mask, 1.0, 0.0).astype(BF16)


def build_routing(routes_ref, scores_ref, place_ref, comb_ref):
    routes = routes_ref[...].astype(F32)
    scores = scores_ref[...]
    weight = scores / jnp.sum(scores, axis=-1, keepdims=True) * route_scale
    spread = one_hot((iota((TOKENS, 128), 1) & 15) == iota((TOKENS, 128), 0))
    spread_t = one_hot((iota((128, TOKENS), 0) & 15) == iota((128, TOKENS), 1))
    eye = one_hot(iota((128, 128), 0) == iota((128, 128), 1))
    lanes = dot_0(routes.astype(BF16), spread)
    earlier = iota((TOKENS, 128), 0) < (iota((TOKENS, 128), 1) & 15)
    ranks = []
    for j in range(TOP):
        hits = jnp.zeros((TOKENS, 128), F32)
        for i in range(TOP):
            same = routes[:, i : i + 1] == lanes[j : j + 1, :]
            hits = hits + jnp.where(same & earlier, 1.0, 0.0)
        ranks.append(jnp.sum(hits, axis=0, keepdims=True))
    rank = jnp.concatenate(ranks, axis=0)
    chunk_lane = (iota((TOP, 128), 1) >> 4).astype(F32)
    code = lanes * 16.0 + chunk_lane * 2.0 + rank
    columns = dot(spread_t, routes.astype(BF16))
    rank_columns = dot_t(eye, rank.astype(BF16))
    weight_columns = dot(spread_t, weight.astype(BF16))
    code_t = columns * 16.0 + (iota((128, TOP), 0) >> 4).astype(F32) * 2.0 + rank_columns

    def place_rows(b, carry):
        at = pl.multiple_of(b * 128, 128)
        row = (iota((128, 128), 0) + at).astype(F32)
        found = row == code[0:1, :]
        for j in range(1, TOP):
            found = found | (row == code[j : j + 1, :])
        place_ref[pl.ds(at, 128), :] = one_hot(found)
        lane = (iota((128, 128), 1) + at).astype(F32)
        mixed = jnp.zeros((128, 128), F32)
        for j in range(TOP):
            mixed = jnp.where(lane == code_t[:, j : j + 1], weight_columns[:, j : j + 1], mixed)
        comb_ref[:, pl.ds(at, 128)] = mixed.astype(BF16)
        return carry

    lax.fori_loop(0, N_DEV * 16 // 128, place_rows, 0)


def layer_kernel(
    nf_ref,
    residual_ref,
    routes_ref,
    scores_ref,
    mix_ref,
    eg_ref,
    eu_ref,
    ed_ref,
    sg_ref,
    su_ref,
    sd_ref,
    dg_ref,
    du_ref,
    dd_ref,
    out_ref,
    place,
    comb,
    eg,
    eu,
    ed,
    sg,
    su,
    sd,
    dw,
    nf,
    snd,
    rcv,
    snd2,
    rcv2,
    acts,
    part,
    parts,
    rows,
    load_sem,
    dense_load_sem,
    dw_send,
    dw_recv,
    fw_send,
    fw_recv,
    a2a_sem,
    ret_sem,
    act_sem,
    part_sem,
):
    me = lax.axis_index("ep")
    lane8 = lax.rem(me, 8)
    group = lax.div(me, 8)
    core = lax.rem(me, 2)
    base8 = group * 8
    sibling = me + 1 - 2 * core

    barrier = pltpu.get_barrier_semaphore()

    def greet(i, carry):
        peer = lax.rem(me + i, N_DEV)
        pl.semaphore_signal(barrier, inc=1, device_id=(peer,), device_id_type=MESH)
        return carry

    lax.fori_loop(1, N_DEV, greet, 0)

    own_rows = pl.ds(pl.multiple_of(lane8 * 32, 32), 32)
    own_loads = [
        pltpu.make_async_copy(src, dw.at[i, own_rows], dense_load_sem.at[i])
        for i, src in enumerate((dg_ref, du_ref, dd_ref))
    ]
    for c in own_loads:
        c.start()
    loads = [
        pltpu.make_async_copy(src, dst, load_sem.at[i])
        for i, (src, dst) in enumerate(
            (
                (sg_ref, sg),
                (su_ref, su),
                (sd_ref, sd),
                (eg_ref.at[0], eg),
                (eu_ref.at[0], eu),
                (ed_ref.at[0], ed),
            )
        )
    ]
    for c in loads:
        c.start()

    build_routing(routes_ref, scores_ref, place, comb)

    for c in own_loads:
        c.wait()
    pl.semaphore_wait(barrier, N_DEV - 1)

    def shard(slot):
        return dw.at[:, pl.ds(pl.multiple_of(slot * 32, 32), 32), :]

    weight_sends = []
    for i in range(4):
        peer = sibling if i == 0 else base8 + lax.rem(lane8 + 2 * i, 8)
        weight_sends.append(
            pltpu.make_async_remote_copy(
                shard(lane8), shard(lane8), dw_send.at[i], dw_recv.at[i],
                device_id=(peer,), device_id_type=MESH,
            )
        )
    nf_value = nf_ref[...]
    nf[...] = nf_value
    stacked = jnp.concatenate([nf_value[:, k * 128 : (k + 1) * 128] for k in range(8)], axis=0)

    def pack(b, carry):
        at = pl.ds(pl.multiple_of(b * 256, 256), 256)
        snd[at, :] = dot(place[at, :], stacked).astype(BF16)
        return carry

    lax.fori_loop(0, 8, pack, 0)

    def tile(ref, index):
        return ref.at[pl.ds(pl.multiple_of(index * 16, 16), 16), :]

    def exchange(source, target, sems):
        def send(i, carry):
            peer = lax.rem(me + i * STEP, N_DEV)
            pltpu.make_async_remote_copy(
                tile(source, peer), tile(target, me), sems.at[0], sems.at[1],
                device_id=(peer,), device_id_type=MESH,
            ).start()
            return carry

        lax.fori_loop(1, N_DEV, send, 0)
        own = pl.ds(pl.multiple_of(me * 16, 16), 16)
        target[own, :] = source[own, :]

    def all_tiles(source, target, sems):
        whole = pl.ds(0, (N_DEV - 1) * 16)
        return pltpu.make_async_remote_copy(
            source.at[whole, :], target.at[whole, :], sems.at[0], sems.at[1],
            device_id=(sibling,), device_id_type=MESH,
        )

    exchange(snd, rcv, a2a_sem)

    act_rows = pl.ds(pl.multiple_of(group * 16, 16), 16)

    def send_acts(i, carry):
        peer = lax.rem(group + i, 16) * 8 + lane8
        pltpu.make_async_remote_copy(
            nf, acts.at[act_rows, :], act_sem.at[0], act_sem.at[1],
            device_id=(peer,), device_id_type=MESH,
        ).start()
        return carry

    lax.fori_loop(1, 16, send_acts, 0)
    acts[act_rows, :] = nf_value
    for c in weight_sends:
        c.start()

    for c in loads[:3]:
        c.wait()
    hidden = (silu(dot(nf_value, sg[...])) * dot(nf_value, su[...])).astype(BF16)
    shared_out = dot(hidden, sd[...])

    rowi = iota((256, 256), 0)
    coli = iota((256, 256), 1)
    swap = one_hot(coli == ((rowi >> 1) & 15) * 16 + (rowi >> 5) * 2 + (rowi & 1))
    swap_t = one_hot(rowi == ((coli >> 1) & 15) * 16 + (coli >> 5) * 2 + (coli & 1))

    for c in loads[3:]:
        c.wait()
    all_tiles(snd, rcv, a2a_sem).wait_recv()
    for b in range(8):
        moved = dot(swap, rcv[b * 256 : (b + 1) * 256, :]).astype(BF16)
        for k in range(8):
            rows[b * 32 : (b + 1) * 32, k * 128 : (k + 1) * 128] = moved[k * 32 : (k + 1) * 32, :]
    taken = rows[...]
    hidden = (silu(dot(taken, eg[...])) * dot(taken, eu[...])).astype(BF16)
    rows[...] = dot(hidden, ed[...]).astype(BF16)
    for b in range(8):
        piece = rows[b * 32 : (b + 1) * 32, :]
        column = jnp.concatenate([piece[:, k * 128 : (k + 1) * 128] for k in range(8)], axis=0)
        snd2[b * 256 : (b + 1) * 256, :] = dot(swap_t, column).astype(BF16)
    exchange(snd2, rcv2, ret_sem)

    forwards = []
    for i in range(1, 4):
        slot = lax.rem(lane8 + 8 - 2 * i, 8)
        pltpu.make_async_remote_copy(
            shard(lane8), shard(slot), dw_send.at[i], dw_recv.at[i],
            device_id=(sibling,), device_id_type=MESH,
        ).wait_recv()
        c = pltpu.make_async_remote_copy(
            shard(slot), shard(slot), fw_send.at[i - 1], fw_recv.at[i - 1],
            device_id=(sibling,), device_id_type=MESH,
        )
        c.start()
        forwards.append(c)
    for c in forwards:
        c.wait_recv()
    weight_sends[0].wait_recv()
    pltpu.make_async_remote_copy(
        acts.at[pl.ds(0, 240), :], acts.at[pl.ds(0, 240), :], act_sem.at[0], act_sem.at[1],
        device_id=(sibling,), device_id_type=MESH,
    ).wait_recv()
    every = acts[...]
    hidden = (silu(dot_t(every, dw[0])) * dot_t(every, dw[1])).astype(BF16)
    part[...] = dot(hidden, dw[2]).astype(BF16)

    def send_parts(i, carry):
        to = lax.rem(group + i, 16)
        pltpu.make_async_remote_copy(
            tile(part, to), tile(parts, group), part_sem.at[0], part_sem.at[1],
            device_id=(to * 8 + lane8,), device_id_type=MESH,
        ).start()
        return carry

    lax.fori_loop(1, 16, send_parts, 0)
    parts[act_rows, :] = part[act_rows, :]

    all_tiles(snd2, rcv2, ret_sem).wait_recv()
    mixed = dot(comb[...], rcv2[...])
    routed = jnp.concatenate([mixed[k * 16 : (k + 1) * 16, :] for k in range(8)], axis=1)
    gate = 1.0 / (1.0 + jnp.exp(-mix_ref[...]))

    all_parts = pltpu.make_async_remote_copy(
        part.at[pl.ds(0, 240), :], parts.at[pl.ds(0, 240), :], part_sem.at[0], part_sem.at[1],
        device_id=(sibling,), device_id_type=MESH,
    )
    all_parts.wait_recv()
    dense = parts[0:16, :].astype(F32)
    for g in range(1, 16):
        dense = dense + parts[g * 16 : (g + 1) * 16, :].astype(F32)
    combined = shared_out + routed + gate * dense
    out_ref[...] = (residual_ref[...] + normed(combined)).astype(BF16)

    for c in weight_sends:
        c.wait_send()
    for c in forwards:
        c.wait_send()
    all_tiles(snd, rcv, a2a_sem).wait_send()
    all_tiles(snd2, rcv2, ret_sem).wait_send()
    for sems in (act_sem,):
        pltpu.make_async_remote_copy(
            acts.at[pl.ds(0, 240), :], acts.at[pl.ds(0, 240), :], sems.at[0], sems.at[1],
            device_id=(sibling,), device_id_type=MESH,
        ).wait_send()
    all_parts.wait_send()


def run_layer(nf, residual, routes, scores, mix, eg, eu, ed, sg, su, sd, dg, du, dd):
    vmem = pl.BlockSpec(memory_space=pltpu.VMEM)
    anywhere = pl.BlockSpec(memory_space=pl.ANY)
    dma = pltpu.SemaphoreType.DMA
    slots = (N_DEV * 16, 128)
    return pl.pallas_call(
        layer_kernel,
        name="layer",
        out_shape=jax.ShapeDtypeStruct((TOKENS, WIDTH), BF16),
        in_specs=[vmem] * 5 + [anywhere] * 9,
        out_specs=vmem,
        scratch_shapes=[
            pltpu.VMEM(slots, BF16),
            pltpu.VMEM((128, N_DEV * 16), BF16),
            pltpu.VMEM((1024, 256), BF16),
            pltpu.VMEM((1024, 256), BF16),
            pltpu.VMEM((256, 1024), BF16),
            pltpu.VMEM((1024, 256), BF16),
            pltpu.VMEM((1024, 256), BF16),
            pltpu.VMEM((256, 1024), BF16),
            pltpu.VMEM((3, 256, 1024), BF16),
            pltpu.VMEM((TOKENS, WIDTH), BF16),
            pltpu.VMEM(slots, BF16),
            pltpu.VMEM(slots, BF16),
            pltpu.VMEM(slots, BF16),
            pltpu.VMEM(slots, BF16),
            pltpu.VMEM((256, 1024), BF16),
            pltpu.VMEM((256, 1024), BF16),
            pltpu.VMEM((256, 1024), BF16),
            pltpu.VMEM((256, 1024), BF16),
            dma((6,)),
            dma((3,)),
            dma((4,)),
            dma((4,)),
            dma((3,)),
            dma((3,)),
            dma((2,)),
            dma((2,)),
            dma((2,)),
            dma((2,)),
        ],
        compiler_params=pltpu.CompilerParams(collective_id=0, has_side_effects=True),
    )(nf, residual, routes, scores, mix, eg, eu, ed, sg, su, sd, dg, du, dd)


def per_device(
    tokens,
    lengths,
    cache_keys,
    cache_values,
    retention_state,
    mix_gain,
    query_weight,
    key_weight,
    value_weight,
    out_weight,
    ffn_gain,
    routes,
    route_scores,
    expert_gate,
    expert_up,
    expert_down,
    shared_gate,
    shared_up,
    shared_down,
    dense_gate,
    dense_up,
    dense_down,
    dense_mix,
):
    residual, new_keys, new_values = retain(
        tokens,
        lengths,
        mix_gain,
        query_weight,
        key_weight,
        value_weight,
        out_weight,
        cache_keys,
        cache_values,
        retention_state,
    )
    normal_ffn = (normed(residual) * ffn_gain).astype(jnp.bfloat16)
    layer_out = run_layer(
        normal_ffn,
        residual,
        routes,
        route_scores,
        dense_mix[None, :],
        expert_gate,
        expert_up,
        expert_down,
        shared_gate,
        shared_up,
        shared_down,
        dense_gate,
        dense_up,
        dense_down,
    )
    return (layer_out, new_keys, new_values)


def solution(mesh):
    in_specs = (
        P("ep", None),
        P("ep"),
        P("ep", None, None),
        P("ep", None, None),
        P("ep", None, None, None),
        P(),
        P(),
        P(),
        P(),
        P(),
        P(),
        P("ep", None),
        P("ep", None),
        P("ep", None, None),
        P("ep", None, None),
        P("ep", None, None),
        P(),
        P(),
        P(),
        P("ep", None),
        P("ep", None),
        P("ep", None),
        P(),
    )
    out_specs = (P("ep", None), P("ep", None), P("ep", None))
    return jax.shard_map(
        per_device, mesh=mesh, in_specs=in_specs, out_specs=out_specs, check_vma=False
    )
```

```python
import math

import jax
import jax.numpy as jnp
from jax import lax
from jax.experimental import pallas as pl
from jax.experimental.pallas import tpu as pltpu
from jax.sharding import PartitionSpec as P

eps = 1e-06
route_scale = 2.5
rope_base = 10000.0
MESH = pl.DeviceIdType.MESH
F32 = jnp.float32
BF16 = jnp.bfloat16
N_DEV = 128
TOKENS = 16
WIDTH = 1024
TOP = 6
STEP = 53


def normed(values):
    return values * lax.rsqrt(jnp.mean(values * values, axis=-1, keepdims=True) + eps)


def dot(a, b):
    return jnp.dot(a, b, preferred_element_type=F32)


def dot_t(a, b):
    return lax.dot_general(a, b, (((1,), (1,)), ((), ())), preferred_element_type=F32)


def silu(v):
    return v / (1.0 + jnp.exp(-v))


def iota(shape, dim):
    return lax.broadcasted_iota(jnp.int32, shape, dim)


def one_hot(mask):
    return jnp.where(mask, 1.0, 0.0).astype(BF16)


def build_routing(routes_ref, scores_ref, place_ref, comb_ref):
    routes_t = routes_ref[...].astype(F32).astype(BF16)
    scores = scores_ref[...]
    weight = (scores / jnp.sum(scores, axis=0, keepdims=True) * route_scale).astype(BF16)
    small_eye = one_hot(iota((TOKENS, TOKENS), 0) == iota((TOKENS, TOKENS), 1))
    routes = dot_t(small_eye, routes_t)
    spread = one_hot((iota((TOKENS, 128), 1) & 15) == iota((TOKENS, 128), 0))
    spread_t = one_hot((iota((128, TOKENS), 0) & 15) == iota((128, TOKENS), 1))
    eye = one_hot(iota((128, 128), 0) == iota((128, 128), 1))
    lanes = dot(routes_t, spread)
    earlier = iota((TOKENS, 128), 0) < (iota((TOKENS, 128), 1) & 15)
    ranks = []
    for j in range(TOP):
        hits = jnp.zeros((TOKENS, 128), F32)
        for i in range(TOP):
            same = routes[:, i : i + 1] == lanes[j : j + 1, :]
            hits = hits + jnp.where(same & earlier, 1.0, 0.0)
        ranks.append(jnp.sum(hits, axis=0, keepdims=True))
    rank = jnp.concatenate(ranks, axis=0)
    chunk_lane = (iota((TOP, 128), 1) >> 4).astype(F32)
    code = lanes * 16.0 + chunk_lane * 2.0 + rank
    columns = dot_t(spread_t, routes_t)
    rank_columns = dot_t(eye, rank.astype(BF16))
    weight_columns = dot_t(spread_t, weight)
    code_t = columns * 16.0 + (iota((128, TOP), 0) >> 4).astype(F32) * 2.0 + rank_columns

    def place_rows(b, carry):
        at = pl.multiple_of(b * 128, 128)
        row = (iota((128, 128), 0) + at).astype(F32)
        found = row == code[0:1, :]
        for j in range(1, TOP):
            found = found | (row == code[j : j + 1, :])
        place_ref[pl.ds(at, 128), :] = one_hot(found)
        lane = (iota((128, 128), 1) + at).astype(F32)
        mixed = jnp.zeros((128, 128), F32)
        for j in range(TOP):
            mixed = jnp.where(lane == code_t[:, j : j + 1], weight_columns[:, j : j + 1], mixed)
        comb_ref[:, pl.ds(at, 128)] = mixed.astype(BF16)
        return carry

    lax.fori_loop(0, N_DEV * 16 // 128, place_rows, 0)


HEADS = 4
DK = 128
DV = 256
LOG_DECAY = [math.log1p(-(2.0 ** (-5 - h))) for h in range(HEADS)]


def rotation(lengths_ref):
    length = lengths_ref[...]
    both = jnp.concatenate([length >> 7, length & 127], axis=0).astype(F32).astype(BF16)
    eye = one_hot(iota((TOKENS, TOKENS), 0) == iota((TOKENS, TOKENS), 1))
    columns = dot_t(eye, both)
    filled = columns[:, 1:2]
    position = columns[:, 0:1] * 128.0 + filled
    place = (iota((TOKENS, DK), 1) & 63).astype(F32)
    angle = position * jnp.exp(place * (-math.log(rope_base) / 64.0))
    sine = jnp.sin(angle)
    signed = jnp.where(iota((TOKENS, DK), 1) < 64, -sine, sine)
    return jnp.cos(angle), signed, filled


def rotated(values, cosine, sine):
    parts = []
    for h in range(HEADS):
        v = values[:, h * DK : (h + 1) * DK]
        parts.append(v * cosine + pltpu.roll(v, 64, axis=1) * sine)
    return jnp.concatenate(parts, axis=1)


def layer_kernel(
    tokens_ref,
    lengths_ref,
    mixg_ref,
    ffng_ref,
    routes_ref,
    scores_ref,
    mix_ref,
    ck_ref,
    cv_ref,
    st_ref,
    wq_ref,
    wk_ref,
    wv_ref,
    wo_ref,
    eg_ref,
    eu_ref,
    ed_ref,
    sg_ref,
    su_ref,
    sd_ref,
    dg_ref,
    du_ref,
    dd_ref,
    out_ref,
    nk_ref,
    nv_ref,
    ck,
    cv,
    st,
    wq,
    wk,
    wv,
    wo,
    kept,
    place,
    comb,
    eg,
    eu,
    ed,
    sg,
    su,
    sd,
    dw,
    nf,
    snd,
    rcv,
    snd2,
    rcv2,
    acts,
    part,
    parts,
    rows,
    load_sem,
    ck_sem,
    cv_sem,
    st_sem,
    dense_load_sem,
    dw_send,
    dw_recv,
    fw_send,
    fw_recv,
    a2a_sem,
    ret_sem,
    act_sem,
    part_sem,
):
    me = lax.axis_index("ep")
    lane8 = lax.rem(me, 8)
    group = lax.div(me, 8)
    core = lax.rem(me, 2)
    base8 = group * 8
    sibling = me + 1 - 2 * core

    barrier = pltpu.get_barrier_semaphore()
    scope = jax.named_scope

    own_rows = pl.ds(pl.multiple_of(lane8 * 32, 32), 32)
    own_loads = [
        pltpu.make_async_copy(src, dw.at[i, own_rows], dense_load_sem.at[i])
        for i, src in enumerate((dg_ref, du_ref, dd_ref))
    ]
    wq_load, wk_load, wv_load, wo_load, *loads = [
        pltpu.make_async_copy(src, dst, load_sem.at[i])
        for i, (src, dst) in enumerate(
            (
                (wq_ref, wq),
                (wk_ref, wk),
                (wv_ref, wv),
                (wo_ref, wo),
                (sg_ref, sg),
                (su_ref, su),
                (sd_ref, sd),
                (eg_ref.at[0], eg),
                (eu_ref.at[0], eu),
                (ed_ref.at[0], ed),
            )
        )
    ]

    def pieces(source, target, sems, count):
        size = TOKENS // count
        return [
            pltpu.make_async_copy(
                source.at[pl.ds(i * size, size)], target.at[pl.ds(i * size, size)], sems.at[i]
            )
            for i in range(count)
        ]

    ck_loads = pieces(ck_ref, ck, ck_sem, 4)
    cv_loads = pieces(cv_ref, cv, cv_sem, 8)
    st_loads = pieces(st_ref, st, st_sem, 8)
    with scope("start"):
        for c in [*own_loads, wq_load, *ck_loads, *st_loads, wk_load, wv_load, *cv_loads, wo_load, *loads]:
            c.start()

        def greet(i, carry):
            peer = lax.rem(me + i, N_DEV)
            pl.semaphore_signal(barrier, inc=1, device_id=(peer,), device_id_type=MESH)
            return carry

        lax.fori_loop(1, N_DEV, greet, 0)

    with scope("routing"):
        build_routing(routes_ref, scores_ref, place, comb)

    def shard(slot):
        return dw.at[:, pl.ds(pl.multiple_of(slot * 32, 32), 32), :]

    with scope("greet_wait"):
        for c in own_loads:
            c.wait()
        pl.semaphore_wait(barrier, N_DEV - 1)
        weight_sends = []
        for i in range(4):
            peer = sibling if i == 0 else base8 + lax.rem(lane8 + 2 * i, 8)
            weight_sends.append(
                pltpu.make_async_remote_copy(
                    shard(lane8), shard(lane8), dw_send.at[i], dw_recv.at[i],
                    device_id=(peer,), device_id_type=MESH,
                )
            )
        for c in weight_sends:
            c.start()

    with scope("query"):
        widened = tokens_ref[...].astype(F32)
        normal_in = (normed(widened) * mixg_ref[...]).astype(BF16)
        cosine, sine, filled = rotation(lengths_ref)
        wq_load.wait()
        queries = (rotated(dot(normal_in, wq[...]), cosine, sine) * DK ** (-0.5)).astype(BF16)
        queries = queries.astype(F32)
        head_of_row = iota((8, HEADS * DK), 0)
        diagonal = head_of_row == (iota((8, HEADS * DK), 1) >> 7)
        spread_queries = [
            jnp.where(diagonal, queries[s : s + 1, :], 0.0).astype(BF16) for s in range(TOKENS)
        ]
        row8 = iota((8, 1), 0)
        decay = jnp.full((8, 1), LOG_DECAY[3], F32)
        for h in range(3):
            decay = jnp.where(row8 == h, LOG_DECAY[h], decay)
        places = iota((8, 128), 1).astype(F32)
    weights = []
    with scope("scores"):
        for i, c in enumerate(ck_loads):
            c.wait()
            for s in range(4 * i, 4 * i + 4):
                live = filled[s : s + 1, :] - places
                score = dot_t(spread_queries[s], ck[s])
                score = score * jnp.exp(jnp.maximum(live, 0.0) * decay)
                weights.append(jnp.where(live > 0.0, score, 0.0).astype(BF16))
    own_block = iota((8, HEADS * DV), 0) == (iota((8, HEADS * DV), 1) >> 8)
    carried = []
    with scope("state"):
        for i, c in enumerate(st_loads):
            c.wait()
            for s in range(2 * i, 2 * i + 2):
                state = st[s].reshape(HEADS * DK, DV).astype(BF16)
                taken = dot(spread_queries[s], state)
                carried.append(taken * jnp.exp((filled[s : s + 1, :] + 1.0) * decay))
    with scope("keys_values"):
        wk_load.wait()
        new_keys = rotated(dot(normal_in, wk[...]), cosine, sine).astype(BF16)
        nk_ref[...] = new_keys
        own = queries * new_keys.astype(F32)
        wv_load.wait()
        new_values = dot(normal_in, wv[...]).astype(BF16)
        nv_ref[...] = new_values
        new_values = new_values.astype(F32)
    with scope("values"):
        for i, c in enumerate(cv_loads):
            c.wait()
            for s in range(2 * i, 2 * i + 2):
                inside = dot(weights[s], cv[s])
                both = inside + jnp.concatenate([carried[s]] * HEADS, axis=1)
                kept[s : s + 1, :] = jnp.sum(jnp.where(own_block, both, 0.0), axis=0, keepdims=True)
    with scope("mix"):
        retained = kept[...]
        heads = []
        for h in range(HEADS):
            strength = jnp.sum(own[:, h * DK : (h + 1) * DK], axis=-1, keepdims=True)
            strength = strength.astype(BF16).astype(F32)
            cut = slice(h * DV, (h + 1) * DV)
            heads.append(normed(retained[:, cut] + strength * new_values[:, cut]).astype(BF16))
        wo_load.wait()
        mixer_out = dot(jnp.concatenate(heads, axis=1), wo[...])
        residual = widened + normed(mixer_out)
        nf_value = (normed(residual) * ffng_ref[...]).astype(BF16)

    with scope("dispatch"):
        nf[...] = nf_value
        stacked = jnp.concatenate([nf_value[:, k * 128 : (k + 1) * 128] for k in range(8)], axis=0)

        def pack(b, carry):
            at = pl.ds(pl.multiple_of(b * 256, 256), 256)
            snd[at, :] = dot(place[at, :], stacked).astype(BF16)
            return carry

        lax.fori_loop(0, 8, pack, 0)

        def tile(ref, index):
            return ref.at[pl.ds(pl.multiple_of(index * 16, 16), 16), :]

        def exchange(source, target, sems):
            def send(i, carry):
                peer = lax.rem(me + i * STEP, N_DEV)
                pltpu.make_async_remote_copy(
                    tile(source, peer), tile(target, me), sems.at[0], sems.at[1],
                    device_id=(peer,), device_id_type=MESH,
                ).start()
                return carry

            lax.fori_loop(1, N_DEV, send, 0)
            own = pl.ds(pl.multiple_of(me * 16, 16), 16)
            target[own, :] = source[own, :]

        def all_tiles(source, target, sems):
            whole = pl.ds(0, (N_DEV - 1) * 16)
            return pltpu.make_async_remote_copy(
                source.at[whole, :], target.at[whole, :], sems.at[0], sems.at[1],
                device_id=(sibling,), device_id_type=MESH,
            )

        exchange(snd, rcv, a2a_sem)

    with scope("acts"):
        act_rows = pl.ds(pl.multiple_of(group * 16, 16), 16)

        def send_acts(i, carry):
            peer = lax.rem(group + i, 16) * 8 + lane8
            pltpu.make_async_remote_copy(
                nf, acts.at[act_rows, :], act_sem.at[0], act_sem.at[1],
                device_id=(peer,), device_id_type=MESH,
            ).start()
            return carry

        lax.fori_loop(1, 16, send_acts, 0)
        acts[act_rows, :] = nf_value
    with scope("shared"):
        for c in loads[:3]:
            c.wait()
        hidden = (silu(dot(nf_value, sg[...])) * dot(nf_value, su[...])).astype(BF16)
        shared_out = dot(hidden, sd[...])

    with scope("swap_build"):
        rowi = iota((256, 256), 0)
        coli = iota((256, 256), 1)
        swap = one_hot(coli == ((rowi >> 1) & 15) * 16 + (rowi >> 5) * 2 + (rowi & 1))
        swap_t = one_hot(rowi == ((coli >> 1) & 15) * 16 + (coli >> 5) * 2 + (coli & 1))

        for c in loads[3:]:
            c.wait()
    with scope("wait_rows"):
        all_tiles(snd, rcv, a2a_sem).wait_recv()
    with scope("experts"):
        for b in range(8):
            moved = dot(swap, rcv[b * 256 : (b + 1) * 256, :]).astype(BF16)
            for k in range(8):
                rows[b * 32 : (b + 1) * 32, k * 128 : (k + 1) * 128] = moved[k * 32 : (k + 1) * 32, :]
        taken = rows[...]
        hidden = (silu(dot(taken, eg[...])) * dot(taken, eu[...])).astype(BF16)
        rows[...] = dot(hidden, ed[...]).astype(BF16)
        for b in range(8):
            piece = rows[b * 32 : (b + 1) * 32, :]
            column = jnp.concatenate([piece[:, k * 128 : (k + 1) * 128] for k in range(8)], axis=0)
            snd2[b * 256 : (b + 1) * 256, :] = dot(swap_t, column).astype(BF16)
    with scope("send_back"):
        exchange(snd2, rcv2, ret_sem)

    with scope("forward"):
        forwards = []
        for i in range(1, 4):
            slot = lax.rem(lane8 + 8 - 2 * i, 8)
            pltpu.make_async_remote_copy(
                shard(lane8), shard(slot), dw_send.at[i], dw_recv.at[i],
                device_id=(sibling,), device_id_type=MESH,
            ).wait_recv()
            c = pltpu.make_async_remote_copy(
                shard(slot), shard(slot), fw_send.at[i - 1], fw_recv.at[i - 1],
                device_id=(sibling,), device_id_type=MESH,
            )
            c.start()
            forwards.append(c)
    with scope("dense_wait"):
        for c in forwards:
            c.wait_recv()
        weight_sends[0].wait_recv()
        pltpu.make_async_remote_copy(
            acts.at[pl.ds(0, 240), :], acts.at[pl.ds(0, 240), :], act_sem.at[0], act_sem.at[1],
            device_id=(sibling,), device_id_type=MESH,
        ).wait_recv()
    with scope("dense"):
        every = acts[...]
        hidden = (silu(dot_t(every, dw[0])) * dot_t(every, dw[1])).astype(BF16)
        part[...] = dot(hidden, dw[2]).astype(BF16)

        def send_parts(i, carry):
            to = lax.rem(group + i, 16)
            pltpu.make_async_remote_copy(
                tile(part, to), tile(parts, group), part_sem.at[0], part_sem.at[1],
                device_id=(to * 8 + lane8,), device_id_type=MESH,
            ).start()
            return carry

        lax.fori_loop(1, 16, send_parts, 0)
        parts[act_rows, :] = part[act_rows, :]

    with scope("wait_back"):
        all_tiles(snd2, rcv2, ret_sem).wait_recv()
    with scope("combine"):
        mixed = dot(comb[...], rcv2[...])
        routed = jnp.concatenate([mixed[k * 16 : (k + 1) * 16, :] for k in range(8)], axis=1)
        gate = 1.0 / (1.0 + jnp.exp(-mix_ref[...]))

        all_parts = pltpu.make_async_remote_copy(
            part.at[pl.ds(0, 240), :], parts.at[pl.ds(0, 240), :], part_sem.at[0], part_sem.at[1],
            device_id=(sibling,), device_id_type=MESH,
        )
    with scope("wait_parts"):
        all_parts.wait_recv()
    with scope("final"):
        dense = parts[0:16, :].astype(F32)
        for g in range(1, 16):
            dense = dense + parts[g * 16 : (g + 1) * 16, :].astype(F32)
        combined = shared_out + routed + gate * dense
        out_ref[...] = (residual + normed(combined)).astype(BF16)

    with scope("drain"):
        for c in weight_sends:
            c.wait_send()
        for c in forwards:
            c.wait_send()
        all_tiles(snd, rcv, a2a_sem).wait_send()
        all_tiles(snd2, rcv2, ret_sem).wait_send()
        for sems in (act_sem,):
            pltpu.make_async_remote_copy(
                acts.at[pl.ds(0, 240), :], acts.at[pl.ds(0, 240), :], sems.at[0], sems.at[1],
                device_id=(sibling,), device_id_type=MESH,
            ).wait_send()
        all_parts.wait_send()


def run_layer(tokens, lengths, mix_gain, ffn_gain, routes, scores, mix, *large):
    vmem = pl.BlockSpec(memory_space=pltpu.VMEM)
    anywhere = pl.BlockSpec(memory_space=pl.ANY)
    dma = pltpu.SemaphoreType.DMA
    slots = (N_DEV * 16, 128)
    return pl.pallas_call(
        layer_kernel,
        name="layer",
        out_shape=(
            jax.ShapeDtypeStruct((TOKENS, WIDTH), BF16),
            jax.ShapeDtypeStruct((TOKENS, HEADS * DK), BF16),
            jax.ShapeDtypeStruct((TOKENS, HEADS * DV), BF16),
        ),
        in_specs=[vmem] * 7 + [anywhere] * 16,
        out_specs=(vmem, vmem, vmem),
        scratch_shapes=[
            pltpu.VMEM((TOKENS, 128, HEADS * DK), BF16),
            pltpu.VMEM((TOKENS, 128, HEADS * DV), BF16),
            pltpu.VMEM((TOKENS, HEADS, DK, DV), F32),
            pltpu.VMEM((WIDTH, HEADS * DK), BF16),
            pltpu.VMEM((WIDTH, HEADS * DK), BF16),
            pltpu.VMEM((WIDTH, HEADS * DV), BF16),
            pltpu.VMEM((HEADS * DV, WIDTH), BF16),
            pltpu.VMEM((TOKENS, HEADS * DV), F32),
            pltpu.VMEM(slots, BF16),
            pltpu.VMEM((128, N_DEV * 16), BF16),
            pltpu.VMEM((1024, 256), BF16),
            pltpu.VMEM((1024, 256), BF16),
            pltpu.VMEM((256, 1024), BF16),
            pltpu.VMEM((1024, 256), BF16),
            pltpu.VMEM((1024, 256), BF16),
            pltpu.VMEM((256, 1024), BF16),
            pltpu.VMEM((3, 256, 1024), BF16),
            pltpu.VMEM((TOKENS, WIDTH), BF16),
            pltpu.VMEM(slots, BF16),
            pltpu.VMEM(slots, BF16),
            pltpu.VMEM(slots, BF16),
            pltpu.VMEM(slots, BF16),
            pltpu.VMEM((256, 1024), BF16),
            pltpu.VMEM((256, 1024), BF16),
            pltpu.VMEM((256, 1024), BF16),
            pltpu.VMEM((256, 1024), BF16),
            dma((10,)),
            dma((4,)),
            dma((8,)),
            dma((8,)),
            dma((3,)),
            dma((4,)),
            dma((4,)),
            dma((3,)),
            dma((3,)),
            dma((2,)),
            dma((2,)),
            dma((2,)),
            dma((2,)),
        ],
        compiler_params=pltpu.CompilerParams(collective_id=0, has_side_effects=True),
    )(tokens, lengths, mix_gain, ffn_gain, routes, scores, mix, *large)


def per_device(
    tokens,
    lengths,
    cache_keys,
    cache_values,
    retention_state,
    mix_gain,
    query_weight,
    key_weight,
    value_weight,
    out_weight,
    ffn_gain,
    routes,
    route_scores,
    expert_gate,
    expert_up,
    expert_down,
    shared_gate,
    shared_up,
    shared_down,
    dense_gate,
    dense_up,
    dense_down,
    dense_mix,
):
    return run_layer(
        tokens,
        lengths[None, :],
        mix_gain[None, :],
        ffn_gain[None, :],
        routes.T,
        route_scores.T,
        dense_mix[None, :],
        cache_keys,
        cache_values,
        retention_state,
        query_weight,
        key_weight,
        value_weight,
        out_weight,
        expert_gate,
        expert_up,
        expert_down,
        shared_gate,
        shared_up,
        shared_down,
        dense_gate,
        dense_up,
        dense_down,
    )


def solution(mesh):
    in_specs = (
        P("ep", None),
        P("ep"),
        P("ep", None, None),
        P("ep", None, None),
        P("ep", None, None, None),
        P(),
        P(),
        P(),
        P(),
        P(),
        P(),
        P("ep", None),
        P("ep", None),
        P("ep", None, None),
        P("ep", None, None),
        P("ep", None, None),
        P(),
        P(),
        P(),
        P("ep", None),
        P("ep", None),
        P("ep", None),
        P(),
    )
    out_specs = (P("ep", None), P("ep", None), P("ep", None))
    return jax.shard_map(
        per_device, mesh=mesh, in_specs=in_specs, out_specs=out_specs, check_vma=False
    )
```

```python
import math

import jax
import jax.numpy as jnp
from jax import lax
from jax.experimental import pallas as pl
from jax.experimental.pallas import tpu as pltpu
from jax.sharding import PartitionSpec as P

eps = 1e-06
route_scale = 2.5
rope_base = 10000.0
MESH = pl.DeviceIdType.MESH
F32 = jnp.float32
BF16 = jnp.bfloat16
N_DEV = 128
TOKENS = 16
WIDTH = 1024
TOP = 6


def normed(values):
    return values * lax.rsqrt(jnp.mean(values * values, axis=-1, keepdims=True) + eps)


def dot(a, b):
    return jnp.dot(a, b, preferred_element_type=F32)


def dot_t(a, b):
    return lax.dot_general(a, b, (((1,), (1,)), ((), ())), preferred_element_type=F32)


def silu(v):
    return v / (1.0 + jnp.exp(-v))


def iota(shape, dim):
    return lax.broadcasted_iota(jnp.int32, shape, dim)


def one_hot(mask):
    return jnp.where(mask, 1.0, 0.0).astype(BF16)


def routing_codes(routes_ref, scores_ref):
    routes_t = routes_ref[...].astype(F32).astype(BF16)
    scores = scores_ref[...]
    weight = (scores / jnp.sum(scores, axis=0, keepdims=True) * route_scale).astype(BF16)
    small_eye = one_hot(iota((TOKENS, TOKENS), 0) == iota((TOKENS, TOKENS), 1))
    spread = one_hot((iota((TOKENS, 128), 1) & 15) == iota((TOKENS, 128), 0))
    spread_t = one_hot((iota((128, TOKENS), 0) & 15) == iota((128, TOKENS), 1))
    eye = one_hot(iota((128, 128), 0) == iota((128, 128), 1))
    routes = dot_t(small_eye, routes_t)
    lanes = dot(routes_t, spread)
    earlier = iota((TOKENS, 128), 0) < (iota((TOKENS, 128), 1) & 15)
    ranks = []
    for j in range(TOP):
        hits = jnp.zeros((TOKENS, 128), F32)
        for i in range(TOP):
            same = routes[:, i : i + 1] == lanes[j : j + 1, :]
            hits = hits + jnp.where(same & earlier, 1.0, 0.0)
        ranks.append(jnp.sum(hits, axis=0, keepdims=True))
    rank = jnp.concatenate(ranks, axis=0)
    code = lanes * 2.0 + rank
    columns = dot_t(spread_t, routes_t)
    rank_columns = dot_t(eye, rank.astype(BF16))
    weight_columns = dot_t(spread_t, weight)
    code_t = columns * 16.0 + (iota((128, TOP), 0) >> 4).astype(F32) * 2.0 + rank_columns
    return code, code_t, weight_columns


def choose_rows(code, choose_ref):
    row = iota((256, 128), 0).astype(F32)
    found = row == code[0:1, :]
    for j in range(1, TOP):
        found = found | (row == code[j : j + 1, :])
    found = found & (iota((256, 128), 1) < TOKENS)
    choose_ref[...] = one_hot(found)


def combine_rows(code_t, weight_columns, comb_ref):
    def fill(b, carry):
        at = pl.multiple_of(b * 128, 128)
        lane = (iota((128, 128), 1) + at).astype(F32)
        mixed = jnp.zeros((128, 128), F32)
        for j in range(TOP):
            mixed = jnp.where(lane == code_t[:, j : j + 1], weight_columns[:, j : j + 1], mixed)
        comb_ref[:, pl.ds(at, 128)] = mixed.astype(BF16)
        return carry

    lax.fori_loop(0, N_DEV * 16 // 128, fill, 0)


HEADS = 4
DK = 128
DV = 256
LOG_DECAY = [math.log1p(-(2.0 ** (-5 - h))) for h in range(HEADS)]


def rotation(lengths_ref):
    length = lengths_ref[...]
    both = jnp.concatenate([length >> 7, length & 127], axis=0).astype(F32).astype(BF16)
    eye = one_hot(iota((TOKENS, TOKENS), 0) == iota((TOKENS, TOKENS), 1))
    columns = dot_t(eye, both)
    filled = columns[:, 1:2]
    position = columns[:, 0:1] * 128.0 + filled
    place = (iota((TOKENS, DK), 1) & 63).astype(F32)
    angle = position * jnp.exp(place * (-math.log(rope_base) / 64.0))
    sine = jnp.sin(angle)
    signed = jnp.where(iota((TOKENS, DK), 1) < 64, -sine, sine)
    return jnp.cos(angle), signed, filled


def rotated(values, cosine, sine):
    parts = []
    for h in range(HEADS):
        v = values[:, h * DK : (h + 1) * DK]
        parts.append(v * cosine + pltpu.roll(v, 64, axis=1) * sine)
    return jnp.concatenate(parts, axis=1)


def layer_kernel(
    tokens_hbm,
    lengths_hbm,
    mixg_hbm,
    ffng_hbm,
    routes_hbm,
    scores_hbm,
    mix_hbm,
    ck_ref,
    cv_ref,
    st_ref,
    wq_ref,
    wk_ref,
    wv_ref,
    wo_ref,
    eg_ref,
    eu_ref,
    ed_ref,
    sg_ref,
    su_ref,
    sd_ref,
    dg_ref,
    du_ref,
    dd_ref,
    out_ref,
    nk_ref,
    nv_ref,
    tokens_ref,
    lengths_ref,
    mixg_ref,
    ffng_ref,
    routes_ref,
    scores_ref,
    mix_ref,
    ck,
    cv,
    st,
    wq,
    wk,
    wv,
    wo,
    kept,
    choose,
    comb,
    swap_t,
    eg,
    eu,
    ed,
    sg,
    su,
    sd,
    dw,
    nf,
    snd,
    rcv,
    snd2,
    rcv2,
    acts,
    part,
    parts,
    rows,
    small_sem,
    load_sem,
    ck_sem,
    cv_sem,
    st_sem,
    dense_load_sem,
    dw_send,
    dw_recv,
    fw_send,
    fw_recv,
    a2a_sem,
    ret_sem,
    act_sem,
    part_sem,
):
    me = lax.axis_index("ep")
    lane8 = lax.rem(me, 8)
    group = lax.div(me, 8)
    core = lax.rem(me, 2)
    base8 = group * 8
    sibling = me + 1 - 2 * core

    barrier = pltpu.get_barrier_semaphore()
    scope = jax.named_scope

    own_rows = pl.ds(pl.multiple_of(lane8 * 32, 32), 32)
    own_loads = [
        pltpu.make_async_copy(src, dw.at[i, own_rows], dense_load_sem.at[i])
        for i, src in enumerate((dg_ref, du_ref, dd_ref))
    ]
    wq_load, wk_load, wv_load, wo_load, *loads = [
        pltpu.make_async_copy(src, dst, load_sem.at[i])
        for i, (src, dst) in enumerate(
            (
                (wq_ref, wq),
                (wk_ref, wk),
                (wv_ref, wv),
                (wo_ref, wo),
                (sg_ref, sg),
                (su_ref, su),
                (sd_ref, sd),
                (eg_ref.at[0], eg),
                (eu_ref.at[0], eu),
                (ed_ref.at[0], ed),
            )
        )
    ]

    def pieces(source, target, sems, count):
        size = TOKENS // count
        return [
            pltpu.make_async_copy(
                source.at[pl.ds(i * size, size)], target.at[pl.ds(i * size, size)], sems.at[i]
            )
            for i in range(count)
        ]

    ck_loads = pieces(ck_ref, ck, ck_sem, 4)
    cv_loads = pieces(cv_ref, cv, cv_sem, 8)
    st_loads = pieces(st_ref, st, st_sem, 8)
    small_loads = [
        pltpu.make_async_copy(src, dst, small_sem.at[i])
        for i, (src, dst) in enumerate(
            (
                (routes_hbm, routes_ref),
                (scores_hbm, scores_ref),
                (tokens_hbm, tokens_ref),
                (lengths_hbm, lengths_ref),
                (mixg_hbm, mixg_ref),
                (ffng_hbm, ffng_ref),
                (mix_hbm, mix_ref),
            )
        )
    ]
    with scope("start"):
        for c in [*small_loads, *own_loads, wq_load, *ck_loads]:
            c.start()

        def greet(b, carry):
            for i in range(16):
                peer = lax.rem(me + b * 16 + i, N_DEV)
                pl.semaphore_signal(barrier, inc=1, device_id=(peer,), device_id_type=MESH)
            return carry

        for i in range(1, 16):
            peer = lax.rem(me + i, N_DEV)
            pl.semaphore_signal(barrier, inc=1, device_id=(peer,), device_id_type=MESH)
        lax.fori_loop(1, 8, greet, 0)

    with scope("routing"):
        rowi = iota((256, 256), 0)
        coli = iota((256, 256), 1)
        swap_t[...] = one_hot(rowi == ((coli >> 1) & 15) * 16 + (coli >> 5) * 2 + (coli & 1))
        for c in small_loads:
            c.wait()
        for c in [wk_load, wv_load, *cv_loads[:4]]:
            c.start()
        code, code_t, weight_columns = routing_codes(routes_ref, scores_ref)
        choose_rows(code, choose)

    def shard(slot):
        return dw.at[:, pl.ds(pl.multiple_of(slot * 32, 32), 32), :]

    with scope("query"):
        widened = tokens_ref[...].astype(F32)
        normal_in = (normed(widened) * mixg_ref[...]).astype(BF16)
        cosine, sine, filled = rotation(lengths_ref)
        wq_load.wait()
        queries = (rotated(dot(normal_in, wq[...]), cosine, sine) * DK ** (-0.5)).astype(BF16)
        queries = queries.astype(F32)
        head_of_row = iota((8, HEADS * DK), 0)
        diagonal = head_of_row == (iota((8, HEADS * DK), 1) >> 7)
        spread_queries = [
            jnp.where(diagonal, queries[s : s + 1, :], 0.0).astype(BF16) for s in range(TOKENS)
        ]
        row8 = iota((8, 1), 0)
        decay = jnp.full((8, 1), LOG_DECAY[3], F32)
        for h in range(3):
            decay = jnp.where(row8 == h, LOG_DECAY[h], decay)
        places = iota((8, 128), 1).astype(F32)
    weights = []
    with scope("scores"):
        for c in [*cv_loads[4:], *st_loads[:4]]:
            c.start()
        for i, c in enumerate(ck_loads):
            c.wait()
            for s in range(4 * i, 4 * i + 4):
                live = filled[s : s + 1, :] - places
                score = dot_t(spread_queries[s], ck[s])
                score = score * jnp.exp(jnp.maximum(live, 0.0) * decay)
                weights.append(jnp.where(live > 0.0, score, 0.0).astype(BF16))
    with scope("keys_values"):
        for c in [*st_loads[4:], wo_load]:
            c.start()
        wk_load.wait()
        new_keys = rotated(dot(normal_in, wk[...]), cosine, sine).astype(BF16)
        nk_ref[...] = new_keys
        own = queries * new_keys.astype(F32)
        wv_load.wait()
        new_values = dot(normal_in, wv[...]).astype(BF16)
        nv_ref[...] = new_values
        new_values = new_values.astype(F32)
    own_block = iota((8, HEADS * DV), 0) == (iota((8, HEADS * DV), 1) >> 8)
    with scope("values"):
        for i, c in enumerate(cv_loads):
            c.wait()
            for s in range(2 * i, 2 * i + 2):
                inside = dot(weights[s], cv[s])
                kept[s : s + 1, :] = jnp.sum(jnp.where(own_block, inside, 0.0), axis=0, keepdims=True)
    with scope("state"):
        for c in loads:
            c.start()
        for i, c in enumerate(st_loads):
            c.wait()
            for s in range(2 * i, 2 * i + 2):
                state = st[s].reshape(HEADS * DK, DV).astype(BF16)
                carried = dot(spread_queries[s], state) * jnp.exp((filled[s : s + 1, :] + 1.0) * decay)
                wide = jnp.concatenate([carried] * HEADS, axis=1)
                kept[s : s + 1, :] += jnp.sum(jnp.where(own_block, wide, 0.0), axis=0, keepdims=True)
    with scope("mix"):
        retained = kept[...]
        heads = []
        for h in range(HEADS):
            strength = jnp.sum(own[:, h * DK : (h + 1) * DK], axis=-1, keepdims=True)
            strength = strength.astype(BF16).astype(F32)
            cut = slice(h * DV, (h + 1) * DV)
            heads.append(normed(retained[:, cut] + strength * new_values[:, cut]).astype(BF16))
        wo_load.wait()
        mixer_out = dot(jnp.concatenate(heads, axis=1), wo[...])
        residual = widened + normed(mixer_out)
        nf_value = (normed(residual) * ffng_ref[...]).astype(BF16)

    def tile(ref, index):
        return ref.at[pl.ds(pl.multiple_of(index * 16, 16), 16), :]

    def exchange(source, target, sems):
        def pack(b):
            block = lax.rem(lax.div(me, 16) + b, 8)
            piece = rows[pl.ds(pl.multiple_of(block * 32, 32), 32), :]
            column = jnp.concatenate([piece[:, k * 128 : (k + 1) * 128] for k in range(8)], axis=0)
            source[pl.ds(pl.multiple_of(block * 256, 256), 256), :] = dot(swap_t[...], column).astype(BF16)

        def send(b, first):
            block = lax.rem(lax.div(me, 16) + b, 8)
            for i in range(first, 16):
                peer = block * 16 + lax.rem(me + i, 16)
                pltpu.make_async_remote_copy(
                    tile(source, peer), tile(target, me), sems.at[0], sems.at[1],
                    device_id=(peer,), device_id_type=MESH,
                ).start()

        def later(b, carry):
            send(b, 0)
            pack(lax.rem(b + 1, 8))
            return carry

        pack(1)
        lax.fori_loop(1, 8, later, 0)
        send(0, 1)
        own = pl.ds(pl.multiple_of(me * 16, 16), 16)
        target[own, :] = source[own, :]

    def all_tiles(source, target, sems):
        whole = pl.ds(0, (N_DEV - 1) * 16)
        return pltpu.make_async_remote_copy(
            source.at[whole, :], target.at[whole, :], sems.at[0], sems.at[1],
            device_id=(sibling,), device_id_type=MESH,
        )

    with scope("greet_wait"):
        for c in own_loads:
            c.wait()
        pl.semaphore_wait(barrier, N_DEV - 1)
        weight_sends = []
        for i in range(4):
            peer = sibling if i == 0 else base8 + lax.rem(lane8 + 2 * i, 8)
            weight_sends.append(
                pltpu.make_async_remote_copy(
                    shard(lane8), shard(lane8), dw_send.at[i], dw_recv.at[i],
                    device_id=(peer,), device_id_type=MESH,
                )
            )

    with scope("dispatch"):
        rows[...] = dot(choose[:, 0:TOKENS], nf_value).astype(BF16)
        exchange(snd, rcv, a2a_sem)

    with scope("acts"):
        nf[...] = nf_value
        act_rows = pl.ds(pl.multiple_of(group * 16, 16), 16)

        def send_acts(i, carry):
            peer = lax.rem(group + i, 16) * 8 + lane8
            pltpu.make_async_remote_copy(
                nf, acts.at[act_rows, :], act_sem.at[0], act_sem.at[1],
                device_id=(peer,), device_id_type=MESH,
            ).start()
            return carry

        lax.fori_loop(1, 16, send_acts, 0)
        acts[act_rows, :] = nf_value
    with scope("weights"):
        for c in weight_sends:
            c.start()
    with scope("shared"):
        for c in loads[:3]:
            c.wait()
        hidden = (silu(dot(nf_value, sg[...])) * dot(nf_value, su[...])).astype(BF16)
        shared_out = dot(hidden, sd[...])

    with scope("swap_build"):
        swap = one_hot(coli == ((rowi >> 1) & 15) * 16 + (rowi >> 5) * 2 + (rowi & 1))
        combine_rows(code_t, weight_columns, comb)
        for c in loads[3:]:
            c.wait()
    with scope("wait_rows"):
        all_tiles(snd, rcv, a2a_sem).wait_recv()
    with scope("experts"):
        for b in range(8):
            moved = dot(swap, rcv[b * 256 : (b + 1) * 256, :]).astype(BF16)
            for k in range(8):
                rows[b * 32 : (b + 1) * 32, k * 128 : (k + 1) * 128] = moved[k * 32 : (k + 1) * 32, :]
        taken = rows[...]
        hidden = (silu(dot(taken, eg[...])) * dot(taken, eu[...])).astype(BF16)
        rows[...] = dot(hidden, ed[...]).astype(BF16)
    with scope("send_back"):
        exchange(snd2, rcv2, ret_sem)

    with scope("forward"):
        forwards = []
        for i in range(1, 4):
            slot = lax.rem(lane8 + 8 - 2 * i, 8)
            pltpu.make_async_remote_copy(
                shard(lane8), shard(slot), dw_send.at[i], dw_recv.at[i],
                device_id=(sibling,), device_id_type=MESH,
            ).wait_recv()
            c = pltpu.make_async_remote_copy(
                shard(slot), shard(slot), fw_send.at[i - 1], fw_recv.at[i - 1],
                device_id=(sibling,), device_id_type=MESH,
            )
            c.start()
            forwards.append(c)
    with scope("dense_wait"):
        for c in forwards:
            c.wait_recv()
        weight_sends[0].wait_recv()
    with scope("acts_wait"):
        pltpu.make_async_remote_copy(
            acts.at[pl.ds(0, 240), :], acts.at[pl.ds(0, 240), :], act_sem.at[0], act_sem.at[1],
            device_id=(sibling,), device_id_type=MESH,
        ).wait_recv()
    with scope("dense"):
        every = acts[...]
        hidden = (silu(dot_t(every, dw[0])) * dot_t(every, dw[1])).astype(BF16)
        part[...] = dot(hidden, dw[2]).astype(BF16)

        def send_parts(i, carry):
            to = lax.rem(group + i, 16)
            pltpu.make_async_remote_copy(
                tile(part, to), tile(parts, group), part_sem.at[0], part_sem.at[1],
                device_id=(to * 8 + lane8,), device_id_type=MESH,
            ).start()
            return carry

        lax.fori_loop(1, 16, send_parts, 0)
        parts[act_rows, :] = part[act_rows, :]

    with scope("wait_parts"):
        all_parts = pltpu.make_async_remote_copy(
            part.at[pl.ds(0, 240), :], parts.at[pl.ds(0, 240), :], part_sem.at[0], part_sem.at[1],
            device_id=(sibling,), device_id_type=MESH,
        )
        all_parts.wait_recv()
        dense = parts[0:16, :].astype(F32)
        for g in range(1, 16):
            dense = dense + parts[g * 16 : (g + 1) * 16, :].astype(F32)
    with scope("wait_back"):
        all_tiles(snd2, rcv2, ret_sem).wait_recv()
    with scope("combine"):
        mixed = dot(comb[...], rcv2[...])
        routed = jnp.concatenate([mixed[k * 16 : (k + 1) * 16, :] for k in range(8)], axis=1)
        gate = 1.0 / (1.0 + jnp.exp(-mix_ref[...]))
    with scope("final"):
        combined = shared_out + routed + gate * dense
        out_ref[...] = (residual + normed(combined)).astype(BF16)

    with scope("drain"):
        for c in weight_sends:
            c.wait_send()
        for c in forwards:
            c.wait_send()
        all_tiles(snd, rcv, a2a_sem).wait_send()
        all_tiles(snd2, rcv2, ret_sem).wait_send()
        for sems in (act_sem,):
            pltpu.make_async_remote_copy(
                acts.at[pl.ds(0, 240), :], acts.at[pl.ds(0, 240), :], sems.at[0], sems.at[1],
                device_id=(sibling,), device_id_type=MESH,
            ).wait_send()
        all_parts.wait_send()


def run_layer(tokens, lengths, mix_gain, ffn_gain, routes, scores, mix, *large):
    vmem = pl.BlockSpec(memory_space=pltpu.VMEM)
    anywhere = pl.BlockSpec(memory_space=pl.ANY)
    dma = pltpu.SemaphoreType.DMA
    slots = (N_DEV * 16, 128)
    return pl.pallas_call(
        layer_kernel,
        name="layer",
        out_shape=(
            jax.ShapeDtypeStruct((TOKENS, WIDTH), BF16),
            jax.ShapeDtypeStruct((TOKENS, HEADS * DK), BF16),
            jax.ShapeDtypeStruct((TOKENS, HEADS * DV), BF16),
        ),
        in_specs=[anywhere] * 23,
        out_specs=(vmem, vmem, vmem),
        scratch_shapes=[
            pltpu.VMEM((TOKENS, WIDTH), BF16),
            pltpu.VMEM((1, TOKENS), jnp.int32),
            pltpu.VMEM((1, WIDTH), F32),
            pltpu.VMEM((1, WIDTH), F32),
            pltpu.VMEM((TOP, TOKENS), jnp.int32),
            pltpu.VMEM((TOP, TOKENS), F32),
            pltpu.VMEM((1, WIDTH), F32),
            pltpu.VMEM((TOKENS, 128, HEADS * DK), BF16),
            pltpu.VMEM((TOKENS, 128, HEADS * DV), BF16),
            pltpu.VMEM((TOKENS, HEADS, DK, DV), F32),
            pltpu.VMEM((WIDTH, HEADS * DK), BF16),
            pltpu.VMEM((WIDTH, HEADS * DK), BF16),
            pltpu.VMEM((WIDTH, HEADS * DV), BF16),
            pltpu.VMEM((HEADS * DV, WIDTH), BF16),
            pltpu.VMEM((TOKENS, HEADS * DV), F32),
            pltpu.VMEM((256, 128), BF16),
            pltpu.VMEM((128, N_DEV * 16), BF16),
            pltpu.VMEM((256, 256), BF16),
            pltpu.VMEM((1024, 256), BF16),
            pltpu.VMEM((1024, 256), BF16),
            pltpu.VMEM((256, 1024), BF16),
            pltpu.VMEM((1024, 256), BF16),
            pltpu.VMEM((1024, 256), BF16),
            pltpu.VMEM((256, 1024), BF16),
            pltpu.VMEM((3, 256, 1024), BF16),
            pltpu.VMEM((TOKENS, WIDTH), BF16),
            pltpu.VMEM(slots, BF16),
            pltpu.VMEM(slots, BF16),
            pltpu.VMEM(slots, BF16),
            pltpu.VMEM(slots, BF16),
            pltpu.VMEM((256, 1024), BF16),
            pltpu.VMEM((256, 1024), BF16),
            pltpu.VMEM((256, 1024), BF16),
            pltpu.VMEM((256, 1024), BF16),
            dma((7,)),
            dma((10,)),
            dma((4,)),
            dma((8,)),
            dma((8,)),
            dma((3,)),
            dma((4,)),
            dma((4,)),
            dma((3,)),
            dma((3,)),
            dma((2,)),
            dma((2,)),
            dma((2,)),
            dma((2,)),
        ],
        compiler_params=pltpu.CompilerParams(collective_id=0, has_side_effects=True),
    )(tokens, lengths, mix_gain, ffn_gain, routes, scores, mix, *large)


def hand_over_kernel(a_ref, b_ref, c_ref, a_out, b_out, c_out):
    a_out[...] = a_ref[...]
    b_out[...] = b_ref[...]
    c_out[...] = c_ref[...]


def hand_over(*arrays):
    vmem = pl.BlockSpec(memory_space=pltpu.VMEM)
    return pl.pallas_call(
        hand_over_kernel,
        name="hand_over",
        out_shape=tuple(jax.ShapeDtypeStruct(a.shape, a.dtype) for a in arrays),
        in_specs=[vmem] * 3,
        out_specs=(vmem,) * 3,
    )(*arrays)


def per_device(
    tokens,
    lengths,
    cache_keys,
    cache_values,
    retention_state,
    mix_gain,
    query_weight,
    key_weight,
    value_weight,
    out_weight,
    ffn_gain,
    routes,
    route_scores,
    expert_gate,
    expert_up,
    expert_down,
    shared_gate,
    shared_up,
    shared_down,
    dense_gate,
    dense_up,
    dense_down,
    dense_mix,
):
    layer_out, new_keys, new_values = run_layer(
        tokens,
        lengths[None, :],
        mix_gain[None, :],
        ffn_gain[None, :],
        routes.T,
        route_scores.T,
        dense_mix[None, :],
        cache_keys,
        cache_values,
        retention_state,
        query_weight,
        key_weight,
        value_weight,
        out_weight,
        expert_gate,
        expert_up,
        expert_down,
        shared_gate,
        shared_up,
        shared_down,
        dense_gate,
        dense_up,
        dense_down,
    )
    return hand_over(layer_out, new_keys, new_values)


def solution(mesh):
    in_specs = (
        P("ep", None),
        P("ep"),
        P("ep", None, None),
        P("ep", None, None),
        P("ep", None, None, None),
        P(),
        P(),
        P(),
        P(),
        P(),
        P(),
        P("ep", None),
        P("ep", None),
        P("ep", None, None),
        P("ep", None, None),
        P("ep", None, None),
        P(),
        P(),
        P(),
        P("ep", None),
        P("ep", None),
        P("ep", None),
        P(),
    )
    out_specs = (P("ep", None), P("ep", None), P("ep", None))
    return jax.shard_map(
        per_device, mesh=mesh, in_specs=in_specs, out_specs=out_specs, check_vma=False
    )
```

```python
import math

import jax
import jax.numpy as jnp
from jax import lax
from jax.experimental import pallas as pl
from jax.experimental.pallas import tpu as pltpu
from jax.sharding import PartitionSpec as P

eps = 1e-06
route_scale = 2.5
rope_base = 10000.0
MESH = pl.DeviceIdType.MESH
F32 = jnp.float32
BF16 = jnp.bfloat16
N_DEV = 128
TOKENS = 16
WIDTH = 1024
TOP = 6


def normed(values):
    return values * lax.rsqrt(jnp.mean(values * values, axis=-1, keepdims=True) + eps)


def dot(a, b):
    return jnp.dot(a, b, preferred_element_type=F32)


def dot_t(a, b):
    return lax.dot_general(a, b, (((1,), (1,)), ((), ())), preferred_element_type=F32)


def silu(v):
    return v / (1.0 + jnp.exp(-v))


def iota(shape, dim):
    return lax.broadcasted_iota(jnp.int32, shape, dim)


def one_hot(mask):
    return jnp.where(mask, 1.0, 0.0).astype(BF16)


def routing_codes(routes_ref):
    routes_t = routes_ref[...].astype(F32).astype(BF16)
    small_eye = one_hot(iota((TOKENS, TOKENS), 0) == iota((TOKENS, TOKENS), 1))
    spread = one_hot((iota((TOKENS, 128), 1) & 15) == iota((TOKENS, 128), 0))
    routes = dot_t(small_eye, routes_t)
    lanes = dot(routes_t, spread)
    earlier = iota((TOKENS, 128), 0) < (iota((TOKENS, 128), 1) & 15)
    ranks = []
    for j in range(TOP):
        hits = jnp.zeros((TOKENS, 128), F32)
        for i in range(TOP):
            same = routes[:, i : i + 1] == lanes[j : j + 1, :]
            hits = hits + jnp.where(same & earlier, 1.0, 0.0)
        ranks.append(jnp.sum(hits, axis=0, keepdims=True))
    rank = jnp.concatenate(ranks, axis=0)
    return lanes * 2.0 + rank, rank


def column_codes(routes_ref, scores_ref, rank):
    routes_t = routes_ref[...].astype(F32).astype(BF16)
    scores = scores_ref[...]
    weight = (scores / jnp.sum(scores, axis=0, keepdims=True) * route_scale).astype(BF16)
    spread_t = one_hot((iota((128, TOKENS), 0) & 15) == iota((128, TOKENS), 1))
    eye = one_hot(iota((128, 128), 0) == iota((128, 128), 1))
    columns = dot_t(spread_t, routes_t)
    rank_columns = dot_t(eye, rank.astype(BF16))
    weight_columns = dot_t(spread_t, weight)
    code_t = columns * 16.0 + (iota((128, TOP), 0) >> 4).astype(F32) * 2.0 + rank_columns
    return code_t, weight_columns


def choose_rows(code, choose_ref):
    row = iota((256, 128), 0).astype(F32)
    found = row == code[0:1, :]
    for j in range(1, TOP):
        found = found | (row == code[j : j + 1, :])
    found = found & (iota((256, 128), 1) < TOKENS)
    choose_ref[...] = one_hot(found)


def combine_rows(code_t, weight_columns, comb_ref):
    def fill(b, carry):
        at = pl.multiple_of(b * 128, 128)
        lane = (iota((128, 128), 1) + at).astype(F32)
        mixed = jnp.zeros((128, 128), F32)
        for j in range(TOP):
            mixed = jnp.where(lane == code_t[:, j : j + 1], weight_columns[:, j : j + 1], mixed)
        comb_ref[:, pl.ds(at, 128)] = mixed.astype(BF16)
        return carry

    lax.fori_loop(0, N_DEV * 16 // 128, fill, 0)


HEADS = 4
DK = 128
DV = 256
LOG_DECAY = [math.log1p(-(2.0 ** (-5 - h))) for h in range(HEADS)]


def rotation(lengths_ref):
    length = lengths_ref[...]
    both = jnp.concatenate([length >> 7, length & 127], axis=0).astype(F32).astype(BF16)
    eye = one_hot(iota((TOKENS, TOKENS), 0) == iota((TOKENS, TOKENS), 1))
    columns = dot_t(eye, both)
    filled = columns[:, 1:2]
    position = columns[:, 0:1] * 128.0 + filled
    place = (iota((TOKENS, DK), 1) & 63).astype(F32)
    angle = position * jnp.exp(place * (-math.log(rope_base) / 64.0))
    sine = jnp.sin(angle)
    signed = jnp.where(iota((TOKENS, DK), 1) < 64, -sine, sine)
    return jnp.cos(angle), signed, filled


def rotated(values, cosine, sine):
    parts = []
    for h in range(HEADS):
        v = values[:, h * DK : (h + 1) * DK]
        parts.append(v * cosine + pltpu.roll(v, 64, axis=1) * sine)
    return jnp.concatenate(parts, axis=1)


def layer_kernel(
    tokens_hbm,
    lengths_hbm,
    mixg_hbm,
    ffng_hbm,
    routes_hbm,
    scores_hbm,
    mix_hbm,
    ck_ref,
    cv_ref,
    st_ref,
    wq_ref,
    wk_ref,
    wv_ref,
    wo_ref,
    eg_ref,
    eu_ref,
    ed_ref,
    sg_ref,
    su_ref,
    sd_ref,
    dg_ref,
    du_ref,
    dd_ref,
    out_ref,
    nk_ref,
    nv_ref,
    tokens_ref,
    lengths_ref,
    mixg_ref,
    ffng_ref,
    routes_ref,
    scores_ref,
    mix_ref,
    ck,
    cv,
    st,
    wq,
    wk,
    wv,
    wo,
    kept,
    choose,
    comb,
    swap_t,
    eg,
    eu,
    ed,
    sg,
    su,
    sd,
    dw,
    nf,
    snd,
    rcv,
    snd2,
    rcv2,
    acts,
    part,
    parts,
    rows,
    small_sem,
    load_sem,
    ck_sem,
    cv_sem,
    st_sem,
    dense_load_sem,
    dw_send,
    dw_recv,
    fw_send,
    fw_recv,
    a2a_sem,
    ret_sem,
    act_sem,
    part_sem,
):
    me = lax.axis_index("ep")
    lane8 = lax.rem(me, 8)
    group = lax.div(me, 8)
    core = lax.rem(me, 2)
    base8 = group * 8
    sibling = me + 1 - 2 * core

    barrier = pltpu.get_barrier_semaphore()
    scope = jax.named_scope

    own_rows = pl.ds(pl.multiple_of(lane8 * 32, 32), 32)
    own_loads = [
        pltpu.make_async_copy(src, dw.at[i, own_rows], dense_load_sem.at[i])
        for i, src in enumerate((dg_ref, du_ref, dd_ref))
    ]
    wq_load, wk_load, wv_load, wo_load, *loads = [
        pltpu.make_async_copy(src, dst, load_sem.at[i])
        for i, (src, dst) in enumerate(
            (
                (wq_ref, wq),
                (wk_ref, wk),
                (wv_ref, wv),
                (wo_ref, wo),
                (sg_ref, sg),
                (su_ref, su),
                (sd_ref, sd),
                (eg_ref.at[0], eg),
                (eu_ref.at[0], eu),
                (ed_ref.at[0], ed),
            )
        )
    ]

    def pieces(source, target, sems, count):
        size = TOKENS // count
        return [
            pltpu.make_async_copy(
                source.at[pl.ds(i * size, size)], target.at[pl.ds(i * size, size)], sems.at[i]
            )
            for i in range(count)
        ]

    ck_loads = pieces(ck_ref, ck, ck_sem, 4)
    cv_loads = pieces(cv_ref, cv, cv_sem, 8)
    st_loads = pieces(st_ref, st, st_sem, 8)
    small_loads = [
        pltpu.make_async_copy(src, dst, small_sem.at[i])
        for i, (src, dst) in enumerate(
            (
                (routes_hbm, routes_ref),
                (scores_hbm, scores_ref),
                (tokens_hbm, tokens_ref),
                (lengths_hbm, lengths_ref),
                (mixg_hbm, mixg_ref),
                (ffng_hbm, ffng_ref),
                (mix_hbm, mix_ref),
            )
        )
    ]
    with scope("start"):
        for c in [*small_loads, *own_loads, wq_load, *ck_loads]:
            c.start()

        def greet(b, carry):
            for i in range(16):
                peer = lax.rem(me + b * 16 + i, N_DEV)
                pl.semaphore_signal(barrier, inc=1, device_id=(peer,), device_id_type=MESH)
            return carry

        for i in range(1, 16):
            peer = lax.rem(me + i, N_DEV)
            pl.semaphore_signal(barrier, inc=1, device_id=(peer,), device_id_type=MESH)
        lax.fori_loop(1, 8, greet, 0)

    with scope("routing"):
        rowi = iota((256, 256), 0)
        coli = iota((256, 256), 1)
        swap_t[...] = one_hot(rowi == ((coli >> 1) & 15) * 16 + (coli >> 5) * 2 + (coli & 1))
        for c in small_loads:
            c.wait()
        for c in [wk_load, wv_load, *cv_loads[:4]]:
            c.start()
        code, rank = routing_codes(routes_ref)
        choose_rows(code, choose)

    def shard(slot):
        return dw.at[:, pl.ds(pl.multiple_of(slot * 32, 32), 32), :]

    with scope("query"):
        widened = tokens_ref[...].astype(F32)
        normal_in = (normed(widened) * mixg_ref[...]).astype(BF16)
        cosine, sine, filled = rotation(lengths_ref)
        wq_load.wait()
        queries = (rotated(dot(normal_in, wq[...]), cosine, sine) * DK ** (-0.5)).astype(BF16)
        queries = queries.astype(F32)
        head_of_row = iota((8, HEADS * DK), 0)
        diagonal = head_of_row == (iota((8, HEADS * DK), 1) >> 7)
        spread_queries = [
            jnp.where(diagonal, queries[s : s + 1, :], 0.0).astype(BF16) for s in range(TOKENS)
        ]
        row8 = iota((8, 1), 0)
        decay = jnp.full((8, 1), LOG_DECAY[3], F32)
        for h in range(3):
            decay = jnp.where(row8 == h, LOG_DECAY[h], decay)
        places = iota((8, 128), 1).astype(F32)
    weights = []
    with scope("scores"):
        for c in [*cv_loads[4:], *st_loads[:4]]:
            c.start()
        for i, c in enumerate(ck_loads):
            c.wait()
            for s in range(4 * i, 4 * i + 4):
                live = filled[s : s + 1, :] - places
                score = dot_t(spread_queries[s], ck[s])
                score = score * jnp.exp(jnp.maximum(live, 0.0) * decay)
                weights.append(jnp.where(live > 0.0, score, 0.0).astype(BF16))
    with scope("keys_values"):
        for c in [*st_loads[4:], wo_load]:
            c.start()
        wk_load.wait()
        new_keys = rotated(dot(normal_in, wk[...]), cosine, sine).astype(BF16)
        nk_ref[...] = new_keys
        own = queries * new_keys.astype(F32)
        wv_load.wait()
        new_values = dot(normal_in, wv[...]).astype(BF16)
        nv_ref[...] = new_values
        new_values = new_values.astype(F32)
    own_block = iota((8, HEADS * DV), 0) == (iota((8, HEADS * DV), 1) >> 8)
    with scope("values"):
        for i, c in enumerate(cv_loads):
            c.wait()
            for s in range(2 * i, 2 * i + 2):
                inside = dot(weights[s], cv[s])
                kept[s : s + 1, :] = jnp.sum(jnp.where(own_block, inside, 0.0), axis=0, keepdims=True)
    with scope("greet_wait"):
        for c in own_loads:
            c.wait()
        pl.semaphore_wait(barrier, N_DEV - 1)
        weight_sends = []
        for which, first in ((slice(0, 1), 0), (slice(1, 3), 4)):
            for i in range(4):
                peer = sibling if i == 0 else base8 + lax.rem(lane8 + 2 * i, 8)
                mine = dw.at[which, pl.ds(pl.multiple_of(lane8 * 32, 32), 32), :]
                weight_sends.append(
                    pltpu.make_async_remote_copy(
                        mine, mine, dw_send.at[first + i], dw_recv.at[first + i],
                        device_id=(peer,), device_id_type=MESH,
                    )
                )
        for c in weight_sends[:4]:
            c.start()
    with scope("state"):
        for c in loads:
            c.start()
        for i, c in enumerate(st_loads):
            c.wait()
            for s in range(2 * i, 2 * i + 2):
                state = st[s].reshape(HEADS * DK, DV).astype(BF16)
                carried = dot(spread_queries[s], state) * jnp.exp((filled[s : s + 1, :] + 1.0) * decay)
                wide = jnp.concatenate([carried] * HEADS, axis=1)
                kept[s : s + 1, :] += jnp.sum(jnp.where(own_block, wide, 0.0), axis=0, keepdims=True)
    with scope("mix"):
        retained = kept[...]
        heads = []
        for h in range(HEADS):
            strength = jnp.sum(own[:, h * DK : (h + 1) * DK], axis=-1, keepdims=True)
            strength = strength.astype(BF16).astype(F32)
            cut = slice(h * DV, (h + 1) * DV)
            heads.append(normed(retained[:, cut] + strength * new_values[:, cut]).astype(BF16))
        wo_load.wait()
        mixer_out = dot(jnp.concatenate(heads, axis=1), wo[...])
        residual = widened + normed(mixer_out)
        nf_value = (normed(residual) * ffng_ref[...]).astype(BF16)

    def tile(ref, index):
        return ref.at[pl.ds(pl.multiple_of(index * 16, 16), 16), :]

    def exchange(source, target, sems):
        def pack(b):
            block = lax.rem(lax.div(me, 16) + b, 8)
            piece = rows[pl.ds(pl.multiple_of(block * 32, 32), 32), :]
            column = jnp.concatenate([piece[:, k * 128 : (k + 1) * 128] for k in range(8)], axis=0)
            source[pl.ds(pl.multiple_of(block * 256, 256), 256), :] = dot(swap_t[...], column).astype(BF16)

        def send(b, first):
            block = lax.rem(lax.div(me, 16) + b, 8)
            for i in range(first, 16):
                peer = block * 16 + lax.rem(me + i, 16)
                pltpu.make_async_remote_copy(
                    tile(source, peer), tile(target, me), sems.at[0], sems.at[1],
                    device_id=(peer,), device_id_type=MESH,
                ).start()

        def later(b, carry):
            send(b, 0)
            pack(lax.rem(b + 1, 8))
            return carry

        pack(1)
        lax.fori_loop(1, 8, later, 0)
        send(0, 1)
        own = pl.ds(pl.multiple_of(me * 16, 16), 16)
        target[own, :] = source[own, :]

    def all_tiles(source, target, sems):
        whole = pl.ds(0, (N_DEV - 1) * 16)
        return pltpu.make_async_remote_copy(
            source.at[whole, :], target.at[whole, :], sems.at[0], sems.at[1],
            device_id=(sibling,), device_id_type=MESH,
        )

    with scope("dispatch"):
        rows[...] = dot(choose[:, 0:TOKENS], nf_value).astype(BF16)
        exchange(snd, rcv, a2a_sem)

    with scope("acts"):
        nf[...] = nf_value
        act_rows = pl.ds(pl.multiple_of(group * 16, 16), 16)

        def send_acts(i, carry):
            peer = lax.rem(group + i, 16) * 8 + lane8
            pltpu.make_async_remote_copy(
                nf, acts.at[act_rows, :], act_sem.at[0], act_sem.at[1],
                device_id=(peer,), device_id_type=MESH,
            ).start()
            return carry

        lax.fori_loop(1, 16, send_acts, 0)
        acts[act_rows, :] = nf_value
    with scope("weights"):
        for c in weight_sends[4:]:
            c.start()
    with scope("shared"):
        for c in loads[:3]:
            c.wait()
        hidden = (silu(dot(nf_value, sg[...])) * dot(nf_value, su[...])).astype(BF16)
        shared_out = dot(hidden, sd[...])

    with scope("swap_build"):
        swap = one_hot(coli == ((rowi >> 1) & 15) * 16 + (rowi >> 5) * 2 + (rowi & 1))
        code_t, weight_columns = column_codes(routes_ref, scores_ref, rank)
        combine_rows(code_t, weight_columns, comb)
        for c in loads[3:]:
            c.wait()
    def forward(which, first):
        for i in range(1, 4):
            slot = lax.rem(lane8 + 8 - 2 * i, 8)
            weight_sends[first + i].wait_recv()
            there = dw.at[which, pl.ds(pl.multiple_of(slot * 32, 32), 32), :]
            c = pltpu.make_async_remote_copy(
                there, there, fw_send.at[first + i], fw_recv.at[first + i],
                device_id=(sibling,), device_id_type=MESH,
            )
            c.start()
            forwards.append(c)

    forwards = []
    with scope("forward_gate"):
        forward(slice(0, 1), 0)
    with scope("wait_rows"):
        all_tiles(snd, rcv, a2a_sem).wait_recv()
    with scope("experts"):
        for b in range(8):
            moved = dot(swap, rcv[b * 256 : (b + 1) * 256, :]).astype(BF16)
            for k in range(8):
                rows[b * 32 : (b + 1) * 32, k * 128 : (k + 1) * 128] = moved[k * 32 : (k + 1) * 32, :]
        taken = rows[...]
        hidden = (silu(dot(taken, eg[...])) * dot(taken, eu[...])).astype(BF16)
        rows[...] = dot(hidden, ed[...]).astype(BF16)
    with scope("send_back"):
        exchange(snd2, rcv2, ret_sem)

    with scope("forward"):
        forward(slice(1, 3), 4)
    with scope("dense_wait"):
        for c in forwards:
            c.wait_recv()
        weight_sends[0].wait_recv()
        weight_sends[4].wait_recv()
    with scope("acts_wait"):
        pltpu.make_async_remote_copy(
            acts.at[pl.ds(0, 240), :], acts.at[pl.ds(0, 240), :], act_sem.at[0], act_sem.at[1],
            device_id=(sibling,), device_id_type=MESH,
        ).wait_recv()
    with scope("dense"):
        every = acts[...]
        hidden = (silu(dot_t(every, dw[0])) * dot_t(every, dw[1])).astype(BF16)
        part[...] = dot(hidden, dw[2]).astype(BF16)

        def send_parts(i, carry):
            to = lax.rem(group + i, 16)
            pltpu.make_async_remote_copy(
                tile(part, to), tile(parts, group), part_sem.at[0], part_sem.at[1],
                device_id=(to * 8 + lane8,), device_id_type=MESH,
            ).start()
            return carry

        lax.fori_loop(1, 16, send_parts, 0)
        parts[act_rows, :] = part[act_rows, :]

    with scope("wait_back"):
        all_tiles(snd2, rcv2, ret_sem).wait_recv()
    with scope("combine"):
        mixed = dot(comb[...], rcv2[...])
        routed = jnp.concatenate([mixed[k * 16 : (k + 1) * 16, :] for k in range(8)], axis=1)
        gate = 1.0 / (1.0 + jnp.exp(-mix_ref[...]))
    with scope("wait_parts"):
        all_parts = pltpu.make_async_remote_copy(
            part.at[pl.ds(0, 240), :], parts.at[pl.ds(0, 240), :], part_sem.at[0], part_sem.at[1],
            device_id=(sibling,), device_id_type=MESH,
        )
        all_parts.wait_recv()
        dense = parts[0:16, :].astype(F32)
        for g in range(1, 16):
            dense = dense + parts[g * 16 : (g + 1) * 16, :].astype(F32)
    with scope("final"):
        combined = shared_out + routed + gate * dense
        out_ref[...] = (residual + normed(combined)).astype(BF16)

    with scope("drain"):
        for c in weight_sends:
            c.wait_send()
        for c in forwards:
            c.wait_send()
        all_tiles(snd, rcv, a2a_sem).wait_send()
        all_tiles(snd2, rcv2, ret_sem).wait_send()
        for sems in (act_sem,):
            pltpu.make_async_remote_copy(
                acts.at[pl.ds(0, 240), :], acts.at[pl.ds(0, 240), :], sems.at[0], sems.at[1],
                device_id=(sibling,), device_id_type=MESH,
            ).wait_send()
        all_parts.wait_send()


def run_layer(tokens, lengths, mix_gain, ffn_gain, routes, scores, mix, *large):
    vmem = pl.BlockSpec(memory_space=pltpu.VMEM)
    anywhere = pl.BlockSpec(memory_space=pl.ANY)
    dma = pltpu.SemaphoreType.DMA
    slots = (N_DEV * 16, 128)
    return pl.pallas_call(
        layer_kernel,
        name="layer",
        out_shape=(
            pltpu.VMEM((TOKENS, WIDTH), BF16),
            pltpu.VMEM((TOKENS, HEADS * DK), BF16),
            pltpu.VMEM((TOKENS, HEADS * DV), BF16),
        ),
        in_specs=[anywhere] * 23,
        out_specs=(vmem, vmem, vmem),
        scratch_shapes=[
            pltpu.VMEM((TOKENS, WIDTH), BF16),
            pltpu.VMEM((1, TOKENS), jnp.int32),
            pltpu.VMEM((1, WIDTH), F32),
            pltpu.VMEM((1, WIDTH), F32),
            pltpu.VMEM((TOP, TOKENS), jnp.int32),
            pltpu.VMEM((TOP, TOKENS), F32),
            pltpu.VMEM((1, WIDTH), F32),
            pltpu.VMEM((TOKENS, 128, HEADS * DK), BF16),
            pltpu.VMEM((TOKENS, 128, HEADS * DV), BF16),
            pltpu.VMEM((TOKENS, HEADS, DK, DV), F32),
            pltpu.VMEM((WIDTH, HEADS * DK), BF16),
            pltpu.VMEM((WIDTH, HEADS * DK), BF16),
            pltpu.VMEM((WIDTH, HEADS * DV), BF16),
            pltpu.VMEM((HEADS * DV, WIDTH), BF16),
            pltpu.VMEM((TOKENS, HEADS * DV), F32),
            pltpu.VMEM((256, 128), BF16),
            pltpu.VMEM((128, N_DEV * 16), BF16),
            pltpu.VMEM((256, 256), BF16),
            pltpu.VMEM((1024, 256), BF16),
            pltpu.VMEM((1024, 256), BF16),
            pltpu.VMEM((256, 1024), BF16),
            pltpu.VMEM((1024, 256), BF16),
            pltpu.VMEM((1024, 256), BF16),
            pltpu.VMEM((256, 1024), BF16),
            pltpu.VMEM((3, 256, 1024), BF16),
            pltpu.VMEM((TOKENS, WIDTH), BF16),
            pltpu.VMEM(slots, BF16),
            pltpu.VMEM(slots, BF16),
            pltpu.VMEM(slots, BF16),
            pltpu.VMEM(slots, BF16),
            pltpu.VMEM((256, 1024), BF16),
            pltpu.VMEM((256, 1024), BF16),
            pltpu.VMEM((256, 1024), BF16),
            pltpu.VMEM((256, 1024), BF16),
            dma((7,)),
            dma((10,)),
            dma((4,)),
            dma((8,)),
            dma((8,)),
            dma((3,)),
            dma((8,)),
            dma((8,)),
            dma((8,)),
            dma((8,)),
            dma((2,)),
            dma((2,)),
            dma((2,)),
            dma((2,)),
        ],
        compiler_params=pltpu.CompilerParams(collective_id=0, has_side_effects=True),
    )(tokens, lengths, mix_gain, ffn_gain, routes, scores, mix, *large)


def hand_over_kernel(a_ref, b_ref, c_ref, a_out, b_out, c_out):
    a_out[...] = a_ref[...]
    b_out[...] = b_ref[...]
    c_out[...] = c_ref[...]


def hand_over(*arrays):
    vmem = pl.BlockSpec(memory_space=pltpu.VMEM)
    return pl.pallas_call(
        hand_over_kernel,
        name="hand_over",
        out_shape=tuple(jax.ShapeDtypeStruct(a.shape, a.dtype) for a in arrays),
        in_specs=[vmem] * 3,
        out_specs=(vmem,) * 3,
    )(*(pltpu.with_memory_space_constraint(a, pltpu.VMEM) for a in arrays))


def per_device(
    tokens,
    lengths,
    cache_keys,
    cache_values,
    retention_state,
    mix_gain,
    query_weight,
    key_weight,
    value_weight,
    out_weight,
    ffn_gain,
    routes,
    route_scores,
    expert_gate,
    expert_up,
    expert_down,
    shared_gate,
    shared_up,
    shared_down,
    dense_gate,
    dense_up,
    dense_down,
    dense_mix,
):
    layer_out, new_keys, new_values = run_layer(
        tokens,
        lengths[None, :],
        mix_gain[None, :],
        ffn_gain[None, :],
        routes.T,
        route_scores.T,
        dense_mix[None, :],
        cache_keys,
        cache_values,
        retention_state,
        query_weight,
        key_weight,
        value_weight,
        out_weight,
        expert_gate,
        expert_up,
        expert_down,
        shared_gate,
        shared_up,
        shared_down,
        dense_gate,
        dense_up,
        dense_down,
    )
    return hand_over(layer_out, new_keys, new_values)


def solution(mesh):
    in_specs = (
        P("ep", None),
        P("ep"),
        P("ep", None, None),
        P("ep", None, None),
        P("ep", None, None, None),
        P(),
        P(),
        P(),
        P(),
        P(),
        P(),
        P("ep", None),
        P("ep", None),
        P("ep", None, None),
        P("ep", None, None),
        P("ep", None, None),
        P(),
        P(),
        P(),
        P("ep", None),
        P("ep", None),
        P("ep", None),
        P(),
    )
    out_specs = (P("ep", None), P("ep", None), P("ep", None))
    return jax.shard_map(
        per_device, mesh=mesh, in_specs=in_specs, out_specs=out_specs, check_vma=False
    )
```

```python
import math

import jax
import jax.numpy as jnp
from jax import lax
from jax.experimental import pallas as pl
from jax.experimental.pallas import tpu as pltpu
from jax.sharding import PartitionSpec as P

eps = 1e-06
route_scale = 2.5
rope_base = 10000.0
MESH = pl.DeviceIdType.MESH
F32 = jnp.float32
BF16 = jnp.bfloat16
N_DEV = 128
TOKENS = 16
WIDTH = 1024
TOP = 6


def normed(values):
    return values * lax.rsqrt(jnp.mean(values * values, axis=-1, keepdims=True) + eps)


def dot(a, b):
    return jnp.dot(a, b, preferred_element_type=F32)


def dot_t(a, b):
    return lax.dot_general(a, b, (((1,), (1,)), ((), ())), preferred_element_type=F32)


def silu(v):
    return v / (1.0 + jnp.exp(-v))


def iota(shape, dim):
    return lax.broadcasted_iota(jnp.int32, shape, dim)


def one_hot(mask):
    return jnp.where(mask, 1.0, 0.0).astype(BF16)


def routing_codes(routes_ref):
    routes_t = routes_ref[...].astype(F32).astype(BF16)
    small_eye = one_hot(iota((TOKENS, TOKENS), 0) == iota((TOKENS, TOKENS), 1))
    spread = one_hot((iota((TOKENS, 128), 1) & 15) == iota((TOKENS, 128), 0))
    routes = dot_t(small_eye, routes_t)
    lanes = dot(routes_t, spread)
    earlier = iota((TOKENS, 128), 0) < (iota((TOKENS, 128), 1) & 15)
    ranks = []
    for j in range(TOP):
        hits = jnp.zeros((TOKENS, 128), F32)
        for i in range(TOP):
            same = routes[:, i : i + 1] == lanes[j : j + 1, :]
            hits = hits + jnp.where(same & earlier, 1.0, 0.0)
        ranks.append(jnp.sum(hits, axis=0, keepdims=True))
    rank = jnp.concatenate(ranks, axis=0)
    return lanes * 2.0 + rank, rank


def column_codes(routes_ref, scores_ref, rank):
    routes_t = routes_ref[...].astype(F32).astype(BF16)
    scores = scores_ref[...]
    weight = (scores / jnp.sum(scores, axis=0, keepdims=True) * route_scale).astype(BF16)
    spread_t = one_hot((iota((128, TOKENS), 0) & 15) == iota((128, TOKENS), 1))
    eye = one_hot(iota((128, 128), 0) == iota((128, 128), 1))
    columns = dot_t(spread_t, routes_t)
    rank_columns = dot_t(eye, rank.astype(BF16))
    weight_columns = dot_t(spread_t, weight)
    code_t = columns * 16.0 + (iota((128, TOP), 0) >> 4).astype(F32) * 2.0 + rank_columns
    return code_t, weight_columns


def choose_rows(code, choose_ref):
    row = iota((256, 128), 0).astype(F32)
    found = row == code[0:1, :]
    for j in range(1, TOP):
        found = found | (row == code[j : j + 1, :])
    found = found & (iota((256, 128), 1) < TOKENS)
    choose_ref[...] = one_hot(found)


def combine_rows(code_t, weight_columns, comb_ref):
    def fill(b, carry):
        at = pl.multiple_of(b * 128, 128)
        lane = (iota((128, 128), 1) + at).astype(F32)
        mixed = jnp.zeros((128, 128), F32)
        for j in range(TOP):
            mixed = jnp.where(lane == code_t[:, j : j + 1], weight_columns[:, j : j + 1], mixed)
        comb_ref[:, pl.ds(at, 128)] = mixed.astype(BF16)
        return carry

    lax.fori_loop(0, N_DEV * 16 // 128, fill, 0)


HEADS = 4
DK = 128
DV = 256
LOG_DECAY = [math.log1p(-(2.0 ** (-5 - h))) for h in range(HEADS)]


def rotation(lengths_ref):
    length = lengths_ref[...]
    both = jnp.concatenate([length >> 7, length & 127], axis=0).astype(F32).astype(BF16)
    eye = one_hot(iota((TOKENS, TOKENS), 0) == iota((TOKENS, TOKENS), 1))
    columns = dot_t(eye, both)
    filled = columns[:, 1:2]
    position = columns[:, 0:1] * 128.0 + filled
    place = (iota((TOKENS, DK), 1) & 63).astype(F32)
    angle = position * jnp.exp(place * (-math.log(rope_base) / 64.0))
    sine = jnp.sin(angle)
    signed = jnp.where(iota((TOKENS, DK), 1) < 64, -sine, sine)
    return jnp.cos(angle), signed, filled


def rotated(values, cosine, sine):
    parts = []
    for h in range(HEADS):
        v = values[:, h * DK : (h + 1) * DK]
        parts.append(v * cosine + pltpu.roll(v, 64, axis=1) * sine)
    return jnp.concatenate(parts, axis=1)


def layer_kernel(
    tokens_hbm,
    lengths_hbm,
    mixg_hbm,
    ffng_hbm,
    routes_hbm,
    scores_hbm,
    mix_hbm,
    ck_ref,
    cv_ref,
    st_ref,
    wq_ref,
    wk_ref,
    wv_ref,
    wo_ref,
    eg_ref,
    eu_ref,
    ed_ref,
    sg_ref,
    su_ref,
    sd_ref,
    dg_ref,
    du_ref,
    dd_ref,
    out_ref,
    nk_ref,
    nv_ref,
    tokens_ref,
    lengths_ref,
    mixg_ref,
    ffng_ref,
    routes_ref,
    scores_ref,
    mix_ref,
    ck,
    cv,
    st,
    wq,
    wk,
    wv,
    wo,
    kept,
    choose,
    comb,
    swap_t,
    eg,
    eu,
    ed,
    sg,
    su,
    sd,
    dw,
    nf,
    snd,
    rcv,
    snd2,
    rcv2,
    acts,
    part,
    parts,
    rows,
    small_sem,
    load_sem,
    ck_sem,
    cv_sem,
    st_sem,
    dense_load_sem,
    dw_send,
    dw_recv,
    fw_send,
    fw_recv,
    a2a_sem,
    ret_sem,
    act_sem,
    part_sem,
):
    me = lax.axis_index("ep")
    lane8 = lax.rem(me, 8)
    group = lax.div(me, 8)
    core = lax.rem(me, 2)
    base8 = group * 8
    sibling = me + 1 - 2 * core

    barrier = pltpu.get_barrier_semaphore()
    scope = jax.named_scope

    own_rows = pl.ds(pl.multiple_of(lane8 * 32, 32), 32)
    own_loads = [
        pltpu.make_async_copy(src, dw.at[i, own_rows], dense_load_sem.at[i])
        for i, src in enumerate((dg_ref, du_ref, dd_ref))
    ]
    wq_load, wk_load, wv_load, wo_load, *loads = [
        pltpu.make_async_copy(src, dst, load_sem.at[i])
        for i, (src, dst) in enumerate(
            (
                (wq_ref, wq),
                (wk_ref, wk),
                (wv_ref, wv),
                (wo_ref, wo),
                (sg_ref, sg),
                (su_ref, su),
                (sd_ref, sd),
                (eg_ref.at[0], eg),
                (eu_ref.at[0], eu),
                (ed_ref.at[0], ed),
            )
        )
    ]

    def pieces(source, target, sems, count):
        size = TOKENS // count
        return [
            pltpu.make_async_copy(
                source.at[pl.ds(i * size, size)], target.at[pl.ds(i * size, size)], sems.at[i]
            )
            for i in range(count)
        ]

    ck_loads = pieces(ck_ref, ck, ck_sem, 4)
    cv_loads = pieces(cv_ref, cv, cv_sem, 8)
    st_loads = pieces(st_ref, st, st_sem, 8)
    small_loads = [
        pltpu.make_async_copy(src, dst, small_sem.at[i])
        for i, (src, dst) in enumerate(
            (
                (routes_hbm, routes_ref),
                (scores_hbm, scores_ref),
                (tokens_hbm, tokens_ref),
                (lengths_hbm, lengths_ref),
                (mixg_hbm, mixg_ref),
                (ffng_hbm, ffng_ref),
                (mix_hbm, mix_ref),
            )
        )
    ]
    with scope("start"):
        for c in [*small_loads, *own_loads, wq_load, *ck_loads]:
            c.start()

        def greet(b, carry):
            for i in range(16):
                peer = lax.rem(me + b * 16 + i, N_DEV)
                pl.semaphore_signal(barrier, inc=1, device_id=(peer,), device_id_type=MESH)
            return carry

        for i in range(1, 16):
            peer = lax.rem(me + i, N_DEV)
            pl.semaphore_signal(barrier, inc=1, device_id=(peer,), device_id_type=MESH)
        lax.fori_loop(1, 8, greet, 0)

    with scope("routing"):
        rowi = iota((256, 256), 0)
        coli = iota((256, 256), 1)
        swap_t[...] = one_hot(rowi == ((coli >> 1) & 15) * 16 + (coli >> 5) * 2 + (coli & 1))
        for c in small_loads:
            c.wait()
        for c in [wk_load, wv_load, *cv_loads[:4]]:
            c.start()
        code, rank = routing_codes(routes_ref)
        choose_rows(code, choose)

    def shard(slot):
        return dw.at[:, pl.ds(pl.multiple_of(slot * 32, 32), 32), :]

    with scope("query"):
        widened = tokens_ref[...].astype(F32)
        normal_in = (normed(widened) * mixg_ref[...]).astype(BF16)
        cosine, sine, filled = rotation(lengths_ref)
        wq_load.wait()
        queries = (rotated(dot(normal_in, wq[...]), cosine, sine) * DK ** (-0.5)).astype(BF16)
        queries = queries.astype(F32)
        head_of_row = iota((8, HEADS * DK), 0)
        diagonal = head_of_row == (iota((8, HEADS * DK), 1) >> 7)
        spread_queries = [
            jnp.where(diagonal, queries[s : s + 1, :], 0.0).astype(BF16) for s in range(TOKENS)
        ]
        row8 = iota((8, 1), 0)
        decay = jnp.full((8, 1), LOG_DECAY[3], F32)
        for h in range(3):
            decay = jnp.where(row8 == h, LOG_DECAY[h], decay)
        places = iota((8, 128), 1).astype(F32)
    weights = []
    with scope("scores"):
        for c in [*cv_loads[4:], *st_loads[:4]]:
            c.start()
        for i, c in enumerate(ck_loads):
            c.wait()
            for s in range(4 * i, 4 * i + 4):
                live = filled[s : s + 1, :] - places
                score = dot_t(spread_queries[s], ck[s])
                score = score * jnp.exp(jnp.maximum(live, 0.0) * decay)
                weights.append(jnp.where(live > 0.0, score, 0.0).astype(BF16))
    with scope("keys_values"):
        for c in [*st_loads[4:], wo_load]:
            c.start()
        wk_load.wait()
        new_keys = rotated(dot(normal_in, wk[...]), cosine, sine).astype(BF16)
        nk_ref[...] = new_keys
        own = queries * new_keys.astype(F32)
        wv_load.wait()
        new_values = dot(normal_in, wv[...]).astype(BF16)
        nv_ref[...] = new_values
        new_values = new_values.astype(F32)
    own_block = iota((8, HEADS * DV), 0) == (iota((8, HEADS * DV), 1) >> 8)
    with scope("values"):
        for i, c in enumerate(cv_loads):
            c.wait()
            for s in range(2 * i, 2 * i + 2):
                inside = dot(weights[s], cv[s])
                kept[s : s + 1, :] = jnp.sum(jnp.where(own_block, inside, 0.0), axis=0, keepdims=True)
    with scope("greet_wait"):
        for c in own_loads:
            c.wait()
        pl.semaphore_wait(barrier, N_DEV - 1)
        weight_sends = []
        for which, first in ((slice(0, 1), 0), (slice(1, 3), 4)):
            for i in range(4):
                peer = sibling if i == 0 else base8 + lax.rem(lane8 + 2 * i, 8)
                mine = dw.at[which, pl.ds(pl.multiple_of(lane8 * 32, 32), 32), :]
                weight_sends.append(
                    pltpu.make_async_remote_copy(
                        mine, mine, dw_send.at[first + i], dw_recv.at[first + i],
                        device_id=(peer,), device_id_type=MESH,
                    )
                )
        for c in weight_sends[:4]:
            c.start()
    with scope("state"):
        for c in loads:
            c.start()
        for i, c in enumerate(st_loads):
            c.wait()
            for s in range(2 * i, 2 * i + 2):
                state = st[s].reshape(HEADS * DK, DV).astype(BF16)
                carried = dot(spread_queries[s], state) * jnp.exp((filled[s : s + 1, :] + 1.0) * decay)
                wide = jnp.concatenate([carried] * HEADS, axis=1)
                kept[s : s + 1, :] += jnp.sum(jnp.where(own_block, wide, 0.0), axis=0, keepdims=True)
    with scope("mix"):
        retained = kept[...]
        heads = []
        for h in range(HEADS):
            strength = jnp.sum(own[:, h * DK : (h + 1) * DK], axis=-1, keepdims=True)
            strength = strength.astype(BF16).astype(F32)
            cut = slice(h * DV, (h + 1) * DV)
            heads.append(normed(retained[:, cut] + strength * new_values[:, cut]).astype(BF16))
        wo_load.wait()
        mixer_out = dot(jnp.concatenate(heads, axis=1), wo[...])
        residual = widened + normed(mixer_out)
        nf_value = (normed(residual) * ffng_ref[...]).astype(BF16)

    def tile(ref, index):
        return ref.at[pl.ds(pl.multiple_of(index * 16, 16), 16), :]

    def exchange(source, target, sems):
        def pack(b):
            block = lax.rem(lax.div(me, 16) + b, 8)
            piece = rows[pl.ds(pl.multiple_of(block * 32, 32), 32), :]
            column = jnp.concatenate([piece[:, k * 128 : (k + 1) * 128] for k in range(8)], axis=0)
            source[pl.ds(pl.multiple_of(block * 256, 256), 256), :] = dot(swap_t[...], column).astype(BF16)

        def send(b, first, late):
            block = lax.rem(lax.div(me, 16) + b, 8)
            for i in range(first, 16):
                peer = block * 16 + lax.rem(me + i, 16)
                pltpu.make_async_remote_copy(
                    tile(source, peer), tile(target, me), sems.at[0], sems.at[late],
                    device_id=(peer,), device_id_type=MESH,
                ).start()

        def step(late):
            def body(b, carry):
                send(b, 0, late)
                pack(lax.rem(b + 1, 8))
                return carry

            return body

        pack(1)
        lax.fori_loop(1, 4, step(1), 0)
        lax.fori_loop(4, 8, step(2), 0)
        send(0, 1, 1)
        own = pl.ds(pl.multiple_of(me * 16, 16), 16)
        target[own, :] = source[own, :]

    def tiles(source, target, sems, count, late):
        whole = pl.ds(0, count * 16)
        return pltpu.make_async_remote_copy(
            source.at[whole, :], target.at[whole, :], sems.at[0], sems.at[late],
            device_id=(sibling,), device_id_type=MESH,
        )

    with scope("dispatch"):
        rows[...] = dot(choose[:, 0:TOKENS], nf_value).astype(BF16)
        exchange(snd, rcv, a2a_sem)

    with scope("acts"):
        nf[...] = nf_value
        act_rows = pl.ds(pl.multiple_of(group * 16, 16), 16)

        def send_acts(i, carry):
            peer = lax.rem(group + i, 16) * 8 + lane8
            pltpu.make_async_remote_copy(
                nf, acts.at[act_rows, :], act_sem.at[0], act_sem.at[1],
                device_id=(peer,), device_id_type=MESH,
            ).start()
            return carry

        lax.fori_loop(1, 16, send_acts, 0)
        acts[act_rows, :] = nf_value
    with scope("weights"):
        for c in weight_sends[4:]:
            c.start()
    with scope("shared"):
        for c in loads[:3]:
            c.wait()
        hidden = (silu(dot(nf_value, sg[...])) * dot(nf_value, su[...])).astype(BF16)
        shared_out = dot(hidden, sd[...])

    with scope("swap_build"):
        swap = one_hot(coli == ((rowi >> 1) & 15) * 16 + (rowi >> 5) * 2 + (rowi & 1))
        code_t, weight_columns = column_codes(routes_ref, scores_ref, rank)
        combine_rows(code_t, weight_columns, comb)
        for c in loads[3:]:
            c.wait()
    def forward(which, first):
        for i in range(1, 4):
            slot = lax.rem(lane8 + 8 - 2 * i, 8)
            weight_sends[first + i].wait_recv()
            there = dw.at[which, pl.ds(pl.multiple_of(slot * 32, 32), 32), :]
            c = pltpu.make_async_remote_copy(
                there, there, fw_send.at[first + i], fw_recv.at[first + i],
                device_id=(sibling,), device_id_type=MESH,
            )
            c.start()
            forwards.append(c)

    forwards = []
    with scope("forward_gate"):
        forward(slice(0, 1), 0)
    def unpack(b):
        block = lax.rem(lax.div(me, 16) + 8 - b, 8)
        moved = dot(swap, rcv[pl.ds(pl.multiple_of(block * 256, 256), 256), :]).astype(BF16)
        at = pl.ds(pl.multiple_of(block * 32, 32), 32)
        for k in range(8):
            rows[at, k * 128 : (k + 1) * 128] = moved[k * 32 : (k + 1) * 32, :]

    with scope("wait_rows"):
        tiles(snd, rcv, a2a_sem, 63, 1).wait_recv()
        for b in range(4):
            unpack(b)
    with scope("wait_rows_far"):
        tiles(snd, rcv, a2a_sem, 64, 2).wait_recv()
    with scope("experts"):
        for b in range(4, 8):
            unpack(b)
        taken = rows[...]
        hidden = (silu(dot(taken, eg[...])) * dot(taken, eu[...])).astype(BF16)
        rows[...] = dot(hidden, ed[...]).astype(BF16)
    with scope("send_back"):
        exchange(snd2, rcv2, ret_sem)

    with scope("forward"):
        forward(slice(1, 3), 4)
    with scope("dense_wait"):
        for c in forwards:
            c.wait_recv()
        weight_sends[0].wait_recv()
        weight_sends[4].wait_recv()
    with scope("acts_wait"):
        pltpu.make_async_remote_copy(
            acts.at[pl.ds(0, 240), :], acts.at[pl.ds(0, 240), :], act_sem.at[0], act_sem.at[1],
            device_id=(sibling,), device_id_type=MESH,
        ).wait_recv()
    with scope("dense"):
        every = acts[...]
        hidden = (silu(dot_t(every, dw[0])) * dot_t(every, dw[1])).astype(BF16)
        part[...] = dot(hidden, dw[2]).astype(BF16)

        def send_parts(i, carry):
            to = lax.rem(group + i, 16)
            pltpu.make_async_remote_copy(
                tile(part, to), tile(parts, group), part_sem.at[0], part_sem.at[1],
                device_id=(to * 8 + lane8,), device_id_type=MESH,
            ).start()
            return carry

        lax.fori_loop(1, 16, send_parts, 0)
        parts[act_rows, :] = part[act_rows, :]

    with scope("wait_back"):
        tiles(snd2, rcv2, ret_sem, 63, 1).wait_recv()
        tiles(snd2, rcv2, ret_sem, 64, 2).wait_recv()
    with scope("combine"):
        mixed = dot(comb[...], rcv2[...])
        routed = jnp.concatenate([mixed[k * 16 : (k + 1) * 16, :] for k in range(8)], axis=1)
        gate = 1.0 / (1.0 + jnp.exp(-mix_ref[...]))
    with scope("wait_parts"):
        all_parts = pltpu.make_async_remote_copy(
            part.at[pl.ds(0, 240), :], parts.at[pl.ds(0, 240), :], part_sem.at[0], part_sem.at[1],
            device_id=(sibling,), device_id_type=MESH,
        )
        all_parts.wait_recv()
        dense = parts[0:16, :].astype(F32)
        for g in range(1, 16):
            dense = dense + parts[g * 16 : (g + 1) * 16, :].astype(F32)
    with scope("final"):
        combined = shared_out + routed + gate * dense
        out_ref[...] = (residual + normed(combined)).astype(BF16)

    with scope("drain"):
        for c in weight_sends:
            c.wait_send()
        for c in forwards:
            c.wait_send()
        tiles(snd, rcv, a2a_sem, N_DEV - 1, 1).wait_send()
        tiles(snd2, rcv2, ret_sem, N_DEV - 1, 1).wait_send()
        for sems in (act_sem,):
            pltpu.make_async_remote_copy(
                acts.at[pl.ds(0, 240), :], acts.at[pl.ds(0, 240), :], sems.at[0], sems.at[1],
                device_id=(sibling,), device_id_type=MESH,
            ).wait_send()
        all_parts.wait_send()


def run_layer(tokens, lengths, mix_gain, ffn_gain, routes, scores, mix, *large):
    vmem = pl.BlockSpec(memory_space=pltpu.VMEM)
    anywhere = pl.BlockSpec(memory_space=pl.ANY)
    dma = pltpu.SemaphoreType.DMA
    slots = (N_DEV * 16, 128)
    return pl.pallas_call(
        layer_kernel,
        name="layer",
        out_shape=(
            pltpu.VMEM((TOKENS, WIDTH), BF16),
            pltpu.VMEM((TOKENS, HEADS * DK), BF16),
            pltpu.VMEM((TOKENS, HEADS * DV), BF16),
        ),
        in_specs=[anywhere] * 23,
        out_specs=(vmem, vmem, vmem),
        scratch_shapes=[
            pltpu.VMEM((TOKENS, WIDTH), BF16),
            pltpu.VMEM((1, TOKENS), jnp.int32),
            pltpu.VMEM((1, WIDTH), F32),
            pltpu.VMEM((1, WIDTH), F32),
            pltpu.VMEM((TOP, TOKENS), jnp.int32),
            pltpu.VMEM((TOP, TOKENS), F32),
            pltpu.VMEM((1, WIDTH), F32),
            pltpu.VMEM((TOKENS, 128, HEADS * DK), BF16),
            pltpu.VMEM((TOKENS, 128, HEADS * DV), BF16),
            pltpu.VMEM((TOKENS, HEADS, DK, DV), F32),
            pltpu.VMEM((WIDTH, HEADS * DK), BF16),
            pltpu.VMEM((WIDTH, HEADS * DK), BF16),
            pltpu.VMEM((WIDTH, HEADS * DV), BF16),
            pltpu.VMEM((HEADS * DV, WIDTH), BF16),
            pltpu.VMEM((TOKENS, HEADS * DV), F32),
            pltpu.VMEM((256, 128), BF16),
            pltpu.VMEM((128, N_DEV * 16), BF16),
            pltpu.VMEM((256, 256), BF16),
            pltpu.VMEM((1024, 256), BF16),
            pltpu.VMEM((1024, 256), BF16),
            pltpu.VMEM((256, 1024), BF16),
            pltpu.VMEM((1024, 256), BF16),
            pltpu.VMEM((1024, 256), BF16),
            pltpu.VMEM((256, 1024), BF16),
            pltpu.VMEM((3, 256, 1024), BF16),
            pltpu.VMEM((TOKENS, WIDTH), BF16),
            pltpu.VMEM(slots, BF16),
            pltpu.VMEM(slots, BF16),
            pltpu.VMEM(slots, BF16),
            pltpu.VMEM(slots, BF16),
            pltpu.VMEM((256, 1024), BF16),
            pltpu.VMEM((256, 1024), BF16),
            pltpu.VMEM((256, 1024), BF16),
            pltpu.VMEM((256, 1024), BF16),
            dma((7,)),
            dma((10,)),
            dma((4,)),
            dma((8,)),
            dma((8,)),
            dma((3,)),
            dma((8,)),
            dma((8,)),
            dma((8,)),
            dma((8,)),
            dma((3,)),
            dma((3,)),
            dma((2,)),
            dma((2,)),
        ],
        compiler_params=pltpu.CompilerParams(collective_id=0, has_side_effects=True),
    )(tokens, lengths, mix_gain, ffn_gain, routes, scores, mix, *large)


def hand_over_kernel(a_ref, b_ref, c_ref, a_out, b_out, c_out, sems):
    copies = [
        pltpu.make_async_copy(source, target, sems.at[i])
        for i, (source, target) in enumerate(((a_ref, a_out), (b_ref, b_out), (c_ref, c_out)))
    ]
    for c in copies:
        c.start()
    for c in copies:
        c.wait()


def hand_over(*arrays):
    vmem = pl.BlockSpec(memory_space=pltpu.VMEM)
    return pl.pallas_call(
        hand_over_kernel,
        name="hand_over",
        out_shape=tuple(jax.ShapeDtypeStruct(a.shape, a.dtype) for a in arrays),
        in_specs=[vmem] * 3,
        out_specs=(pl.BlockSpec(memory_space=pltpu.HBM),) * 3,
        scratch_shapes=[pltpu.SemaphoreType.DMA((3,))],
    )(*(pltpu.with_memory_space_constraint(a, pltpu.VMEM) for a in arrays))


def per_device(
    tokens,
    lengths,
    cache_keys,
    cache_values,
    retention_state,
    mix_gain,
    query_weight,
    key_weight,
    value_weight,
    out_weight,
    ffn_gain,
    routes,
    route_scores,
    expert_gate,
    expert_up,
    expert_down,
    shared_gate,
    shared_up,
    shared_down,
    dense_gate,
    dense_up,
    dense_down,
    dense_mix,
):
    layer_out, new_keys, new_values = run_layer(
        tokens,
        lengths[None, :],
        mix_gain[None, :],
        ffn_gain[None, :],
        routes.T,
        route_scores.T,
        dense_mix[None, :],
        cache_keys,
        cache_values,
        retention_state,
        query_weight,
        key_weight,
        value_weight,
        out_weight,
        expert_gate,
        expert_up,
        expert_down,
        shared_gate,
        shared_up,
        shared_down,
        dense_gate,
        dense_up,
        dense_down,
    )
    return hand_over(layer_out, new_keys, new_values)


def solution(mesh):
    in_specs = (
        P("ep", None),
        P("ep"),
        P("ep", None, None),
        P("ep", None, None),
        P("ep", None, None, None),
        P(),
        P(),
        P(),
        P(),
        P(),
        P(),
        P("ep", None),
        P("ep", None),
        P("ep", None, None),
        P("ep", None, None),
        P("ep", None, None),
        P(),
        P(),
        P(),
        P("ep", None),
        P("ep", None),
        P("ep", None),
        P(),
    )
    out_specs = (P("ep", None), P("ep", None), P("ep", None))
    return jax.shard_map(
        per_device, mesh=mesh, in_specs=in_specs, out_specs=out_specs, check_vma=False
    )
```
